32 devices in a mesh: grp: 2 (over y), ep: 4 (over z), tp: 4 (over x, core).
Axes of the slice: x: 2, y: 2, z: 4, core: 2. Of those that a mesh axis runs over, the one named last changes fastest.
Arguments:
- queries: bfloat16 [4096, 1024], P(('grp', 'ep'), 'tp'), parts along dimension 0, may hold values from -6 to 6
- key_rows: bfloat16 [4096, 512], P(('grp', 'ep'), 'tp'), parts along dimension 0, may hold values from -6 to 6
- value_rows: bfloat16 [4096, 512], P(('grp', 'ep'), 'tp'), parts along dimension 0, may hold values from -6 to 6
- query_gain: float32 [128], replicated, may hold values from 0.3 to 9
- key_gain: float32 [128], replicated, may hold values from 0.3 to 9
- log_forget: float32 [8, 4096], P('tp', 'grp'), parts along dimension 1, may hold values from -2048 to 0, as said below
- out_weight: bfloat16 [1024, 2048], P('tp'), may hold values from -0.1875 to 0.1875
- expert_rows: bfloat16 [4096, 2048], P(('grp', 'ep')), parts along dimension 0, may hold values from -6 to 6
- expert_gain: float32 [2048], replicated, may hold values from 0.1 to 1.9
- routes: int32 [2, 4096], P(None, ('grp', 'ep')), parts along dimension 1, may hold values from 0 to 31, as said below
- route_weight: float32 [2, 4096], P(None, ('grp', 'ep')), parts along dimension 1, may hold values from 0.1 to 1
- gate_weight: bfloat16 [32, 2048, 1024], P('ep', None, 'tp'), may hold values from -0.125 to 0.125
- up_weight: bfloat16 [32, 2048, 1024], P('ep', None, 'tp'), may hold values from -0.125 to 0.125
- down_weight: bfloat16 [32, 1024, 2048], P('ep', 'tp'), may hold values from -0.1875 to 0.1875
Outputs:
- mixer_out: bfloat16 [4096, 2048], P(('grp', 'ep', 'tp')), parts along dimension 0
- expert_out: bfloat16 [4096, 2048], P(('grp', 'ep'), 'tp'), parts along dimension 0
The draws below stay inside these ranges and needn't reach their ends.
There are 2 independent parts, one for each index of `grp`. The reference program is written for one: setup_inputs(seed, part) draws one part's arguments, and reference() takes and returns one part's arrays. A program takes and returns all parts, laid end to end along the dimension named above; an argument that names none is the same for every part. Nothing has to cross between parts.
Inputs may be any that keep to these rules, and one draw needn't show every extreme that they name: `log_forget`: each head's values never rise along the positions. `routes`: the 2 experts of a token differ and lie in one group of 8 consecutive numbers. Among the tokens of one index of ep (512 consecutive tokens), no expert is named more than 48 times, and in every draw some experts are named exactly 48 times in every such block.
All inputs are finite; a program needn't handle non-finite values.
Results may differ from the reference program's by a relative error of at most 0.012.
The reference program's roundings to bfloat16 on the way count: a program that leaves them out, or rounds other values in their place, can miss the bound.
Values may be sent and summed in bfloat16 or wider, within the bound.
A program may use at most 128 MiB of HBM per device.

```python
import math
import jax
import jax.numpy as jnp
from jax import lax

D = 2048
QUERY_HEADS = 8
KV_HEADS = 4
HEAD_SIZE = 128
EXPERTS = 32
GROUP_SIZE = 8
FF = 1024
TOP = 2
SPAN = 512
SEQUENCE_TOKENS = 2048
CAP = 48
N_EP = 4
N_TP = 4


def gain_draw(gain_key):
    return jnp.clip(1.0 + 0.18 * jax.random.normal(gain_key, (HEAD_SIZE,), jnp.float32), 0.3, 1.7)


def draw_query_gain(key, part):
    return gain_draw(jax.random.fold_in(key, 3))


def draw_key_gain(key, part):
    return gain_draw(jax.random.fold_in(key, 5))


def draw_log_forget(key, part):
    divided_keys = jax.random.split(jax.random.fold_in(key, 7), 7)
    token_position = jnp.arange(SEQUENCE_TOKENS, dtype=jnp.int32)
    shard_factor = jnp.exp(jax.random.uniform(divided_keys[0], (SEQUENCE_TOKENS // SPAN,), jnp.float32, -0.7, 0.7))
    factor_vector = jnp.repeat(shard_factor, SPAN)
    fast_rank = jax.random.permutation(divided_keys[1], QUERY_HEADS).astype(jnp.int32)
    is_fast = fast_rank < QUERY_HEADS // 2
    slow_rate = jax.random.uniform(divided_keys[2], (QUERY_HEADS,), jnp.float32, 0.3, 0.9) / SEQUENCE_TOKENS
    fast_rate = 1.0 / jax.random.uniform(divided_keys[3], (QUERY_HEADS,), jnp.float32, 30.0, 50.0)
    baseline_rate = jnp.where(is_fast, fast_rate, slow_rate)
    jitter_amount = jax.random.uniform(divided_keys[4], (QUERY_HEADS, SEQUENCE_TOKENS), jnp.float32, 0.5, 1.5)
    spike_position = jax.random.randint(divided_keys[5], (QUERY_HEADS, 3), 0, SEQUENCE_TOKENS)
    spike_length = -jnp.log(jax.random.uniform(divided_keys[6], (QUERY_HEADS, 3), jnp.float32, 0.6, 0.8))
    spike_events = jnp.sum(jnp.where(token_position[None, None, :] == spike_position[:, :, None], spike_length[:, :, None], 0.0), axis=1)
    logarithm_step = -(baseline_rate[:, None] * factor_vector[None, :] * jitter_amount + spike_events)
    return jnp.cumsum(logarithm_step, axis=1)


def route_block(block_key, full_group):
    divided_keys = jax.random.split(block_key, 4)
    full_rows = GROUP_SIZE * CAP // 2
    rest_rows = SPAN - full_rows
    other_sizes = jnp.array([rest_rows // 2, rest_rows // 3, rest_rows - rest_rows // 2 - rest_rows // 3], jnp.int32)
    others = (full_group + 1 + jax.random.permutation(divided_keys[0], 3).astype(jnp.int32)) % 4
    group_sizes = jnp.zeros((4,), jnp.int32).at[full_group].set(full_rows).at[others].set(other_sizes)
    group_ends = jnp.cumsum(group_sizes)
    token_position = jnp.arange(SPAN, dtype=jnp.int32)
    group_of = jnp.sum((token_position[:, None] >= group_ends[None, :]).astype(jnp.int32), axis=1)
    within = token_position - (group_ends - group_sizes)[group_of]
    orders = jax.vmap(lambda sub_key: jax.random.permutation(sub_key, GROUP_SIZE).astype(jnp.int32))(jax.random.split(divided_keys[1], 4))
    shifts = jax.random.randint(divided_keys[2], (4,), 0, GROUP_SIZE - 1)
    first_pick = orders[group_of, within % GROUP_SIZE]
    second_pick = orders[group_of, (within + 1 + (within // GROUP_SIZE + shifts[group_of]) % (GROUP_SIZE - 1)) % GROUP_SIZE]
    chosen = jnp.stack([group_of * GROUP_SIZE + first_pick, group_of * GROUP_SIZE + second_pick])
    shuffle = jax.random.permutation(divided_keys[3], SPAN)
    return chosen[:, shuffle]


def draw_routes(key, part):
    full_group = jax.random.randint(jax.random.fold_in(key, 11), (), 0, 4)
    block_keys = jax.random.split(jax.random.fold_in(key, 12), SEQUENCE_TOKENS // SPAN)
    blocks = jax.vmap(lambda block_key: route_block(block_key, full_group))(block_keys)
    return jnp.transpose(blocks, (1, 0, 2)).reshape(2, SEQUENCE_TOKENS).astype(jnp.int32)


def steps_of(key, dims, cuts, smallest, high):
    def one(position, parts):
        draws = jax.random.uniform(jax.random.fold_in(jax.random.fold_in(key, 6), position), (parts,), jnp.float32, smallest / len(cuts), high / len(cuts))
        return jnp.repeat(jnp.exp(draws), dims[position] // parts).reshape((-1,) + (1,) * (len(dims) - position - 1))

    factor_of = one(*cuts[0])
    for cut in cuts[1:]:
        factor_of = factor_of * one(*cut)
    return factor_of


def noise(rng, shape, spread, bound, cuts=(), held_as=jnp.bfloat16):
    result = jax.random.normal(rng, shape, jnp.float32) * spread
    if len(cuts) > 0:
        result = steps_of(rng, shape, cuts, -0.22, 0.18) * result
    return jnp.clip(result, min=-bound, max=bound).astype(held_as)


def setup_inputs(seed: int = 0, part: int = 0) -> dict:
    keys = jax.random.split(jax.random.key(seed), 15)
    part_keys = jax.random.split(jax.random.fold_in(keys[14], part), 15)
    return {
        "queries": noise(part_keys[0], (SEQUENCE_TOKENS, QUERY_HEADS * HEAD_SIZE), 1.0, 6.0, ((0, 4), (1, 4))),
        "key_rows": noise(part_keys[1], (SEQUENCE_TOKENS, KV_HEADS * HEAD_SIZE), 1.0, 6.0, ((0, 4), (1, 4))),
        "value_rows": noise(part_keys[2], (SEQUENCE_TOKENS, KV_HEADS * HEAD_SIZE), 1.0, 6.0, ((0, 4), (1, 4))),
        "query_gain": draw_query_gain(jax.random.fold_in(keys[14], 71), part),
        "key_gain": draw_key_gain(jax.random.fold_in(keys[14], 71), part),
        "log_forget": draw_log_forget(jax.random.fold_in(jax.random.fold_in(keys[14], part), 71), part),
        "out_weight": noise(keys[6], (QUERY_HEADS * HEAD_SIZE, D), (QUERY_HEADS * HEAD_SIZE) ** -0.5, 0.1875, ((0, 4),)),
        "expert_rows": noise(part_keys[7], (SEQUENCE_TOKENS, D), 1.0, 6.0, ((0, 4),)),
        "expert_gain": jnp.clip(1.0 + 0.18 * jax.random.normal(keys[8], (D,), jnp.float32), 0.1, 1.9),
        "routes": draw_routes(jax.random.fold_in(jax.random.fold_in(keys[14], part), 71), part),
        "route_weight": jnp.clip(jnp.exp(math.log(1.0) - 2.3025851 * jax.random.uniform(part_keys[10], (TOP, SEQUENCE_TOKENS), jnp.float32) ** steps_of(part_keys[10], (TOP, SEQUENCE_TOKENS), ((1, 4),), -0.2, 0.2)), 0.1, 1.0),
        "gate_weight": noise(keys[11], (EXPERTS, D, FF), D ** -0.5, 0.125, ((0, 4), (2, 4))),
        "up_weight": noise(keys[12], (EXPERTS, D, FF), D ** -0.5, 0.125, ((0, 4), (2, 4))),
        "down_weight": noise(keys[13], (EXPERTS, FF, D), FF ** -0.5, 0.1875, ((0, 4), (1, 4))),
    }


def head_norm(inputs, scale_gain):
    widened = inputs.astype(jnp.float32)
    factor = lax.rsqrt(lax.optimization_barrier(jnp.mean(widened * widened, axis=-1, keepdims=True)) + 1e-06)
    return widened * factor * scale_gain.astype(jnp.float32)

def slot_table(chosen, experts_all, capacity):
    n_rows = chosen.shape[0]
    per_row = chosen.shape[1]
    flat_ids = chosen.reshape(-1)
    one_hot = (flat_ids[:, None] == jnp.arange(experts_all, dtype=jnp.int32)[None, :]).astype(jnp.int32)
    within = lax.optimization_barrier(jnp.sum((jnp.cumsum(one_hot, axis=0) - 1) * one_hot, axis=1))
    slot_index = (flat_ids * capacity + within).astype(jnp.int32)
    row_of = jnp.arange(n_rows * per_row, dtype=jnp.int32) // per_row
    slot_owner = jnp.full((experts_all * capacity,), n_rows, jnp.int32).at[slot_index].set(row_of)
    return (slot_index.reshape(n_rows, per_row), slot_owner)

def reference(queries, key_rows, value_rows, query_gain, key_gain, log_forget, out_weight, expert_rows, expert_gain, routes, route_weight, gate_weight, up_weight, down_weight):
    span_len = SEQUENCE_TOKENS // N_EP
    group_ratio = QUERY_HEADS // KV_HEADS
    scale_qk = HEAD_SIZE ** (-0.5)
    q_all = lax.optimization_barrier(head_norm(queries.reshape(SEQUENCE_TOKENS, KV_HEADS, group_ratio, HEAD_SIZE), query_gain).astype(jnp.bfloat16)).astype(jnp.float32)
    k_all = lax.optimization_barrier(head_norm(key_rows.reshape(SEQUENCE_TOKENS, KV_HEADS, HEAD_SIZE), key_gain).astype(jnp.bfloat16)).astype(jnp.float32)
    v_all = value_rows.reshape(SEQUENCE_TOKENS, KV_HEADS, HEAD_SIZE).astype(jnp.float32)
    positions = jnp.arange(span_len, dtype=jnp.int32)

    def query_block(block_index):
        q_here = lax.dynamic_slice_in_dim(q_all, block_index * span_len, span_len, 0)
        gates_here = lax.dynamic_slice_in_dim(log_forget, block_index * span_len, span_len, 1)
        gates_here = gates_here.T.reshape(span_len, KV_HEADS, group_ratio)

        def key_step(key_index, running):
            run_max, run_sum, run_acc = running
            k_here = lax.dynamic_slice_in_dim(k_all, key_index * span_len, span_len, 0)
            v_here = lax.dynamic_slice_in_dim(v_all, key_index * span_len, span_len, 0)
            key_gates = lax.dynamic_slice_in_dim(log_forget, key_index * span_len, span_len, 1)
            key_gates = key_gates.reshape(KV_HEADS, group_ratio, span_len)
            scores = jnp.einsum('qgrd,kgd->qgrk', q_here, k_here) * scale_qk
            scores = scores + gates_here[..., None] - key_gates[None]
            visible = (key_index * span_len + positions)[None, :] <= (block_index * span_len + positions)[:, None]
            scores = jnp.where(visible[:, None, None, :], scores, -jnp.inf)
            new_max = jnp.maximum(run_max, lax.optimization_barrier(jnp.max(scores, axis=-1)))
            shrink = jnp.exp(run_max - new_max)
            weights = jnp.exp(scores - new_max[..., None])
            run_sum = shrink * run_sum + lax.optimization_barrier(jnp.sum(weights, axis=-1))
            weights_low = lax.optimization_barrier(weights.astype(jnp.bfloat16)).astype(jnp.float32)
            gathered = jnp.einsum('qgrk,kgd->qgrd', weights_low, v_here)
            return (new_max, run_sum, shrink[..., None] * run_acc + gathered)
        start_state = (jnp.full((span_len, KV_HEADS, group_ratio), -jnp.inf, jnp.float32), jnp.zeros((span_len, KV_HEADS, group_ratio), jnp.float32), jnp.zeros((span_len, KV_HEADS, group_ratio, HEAD_SIZE), jnp.float32))
        run_max, run_sum, run_acc = lax.fori_loop(0, block_index + 1, key_step, start_state)
        return (run_acc / run_sum[..., None]).astype(jnp.bfloat16)
    attended = lax.map(query_block, jnp.arange(N_EP, dtype=jnp.int32))
    attended = attended.reshape(SEQUENCE_TOKENS, QUERY_HEADS * HEAD_SIZE)
    mixer_out = jnp.dot(attended, out_weight, preferred_element_type=jnp.float32).astype(jnp.bfloat16)
    normed = head_norm(expert_rows, expert_gain).astype(jnp.bfloat16)
    block_routes = routes.reshape(TOP, N_EP, span_len).transpose(1, 2, 0)
    slot_all, owner_all = jax.vmap(lambda chosen: slot_table(chosen, EXPERTS, CAP))(block_routes)
    block_base = jnp.arange(N_EP, dtype=jnp.int32)[:, None] * span_len
    global_rows = jnp.where(owner_all == span_len, SEQUENCE_TOKENS, owner_all + block_base).astype(jnp.int32)
    row_index = global_rows.reshape(N_EP, EXPERTS, CAP).transpose(1, 0, 2).reshape(EXPERTS, N_EP * CAP)
    padded = jnp.concatenate([normed, jnp.zeros((1, D), jnp.bfloat16)], axis=0)
    ff_part = FF // N_TP

    def one_expert(inputs):
        index_rows, w_gate, w_up, w_down = inputs
        taken = padded[index_rows]
        gate_part = jnp.dot(taken, w_gate, preferred_element_type=jnp.float32)
        up_part = jnp.dot(taken, w_up, preferred_element_type=jnp.float32)
        hidden = (jax.nn.silu(gate_part) * up_part).astype(jnp.bfloat16)
        running = jnp.zeros((N_EP * CAP, D), jnp.float32)
        for part_index in range(N_TP):
            piece = jnp.dot(hidden[:, part_index * ff_part:(part_index + 1) * ff_part], w_down[part_index * ff_part:(part_index + 1) * ff_part], preferred_element_type=jnp.float32)
            running = running + lax.optimization_barrier(piece.astype(jnp.bfloat16)).astype(jnp.float32)
        return running.astype(jnp.bfloat16)
    results = lax.map(one_expert, (row_index, gate_weight, up_weight, down_weight))
    result_table = results.reshape(EXPERTS, N_EP, CAP, D)
    expert_of = slot_all // CAP
    cell_of = slot_all % CAP
    block_id = jnp.arange(N_EP, dtype=jnp.int32)[:, None, None]
    picked = result_table[expert_of, block_id, cell_of]
    weights_all = route_weight.reshape(TOP, N_EP, span_len).transpose(1, 2, 0)
    expert_out = lax.optimization_barrier(jnp.sum(picked.astype(jnp.float32) * weights_all[..., None], axis=2))
    expert_out = expert_out.astype(jnp.bfloat16).reshape(SEQUENCE_TOKENS, D)
    return (mixer_out, expert_out)
```

```python
import functools

import jax
import jax.numpy as jnp
from jax import lax
from jax.experimental import pallas as pl
from jax.experimental.pallas import tpu as pltpu
from jax.sharding import PartitionSpec as P

HEAD_SIZE = 128
EXPERTS = 32
TOP = 2
GROUP_SIZE = 8
VMEM_LIMIT = 65000 * 1024


def head_norm(inputs, scale_gain):
    widened = inputs.astype(jnp.float32)
    factor = lax.rsqrt(jnp.mean(widened * widened, axis=-1, keepdims=True) + 1e-06)
    return widened * factor * scale_gain


def slot_table(chosen, experts_all, capacity):
    n_rows = chosen.shape[0]
    per_row = chosen.shape[1]
    flat_ids = chosen.reshape(-1)
    one_hot = (flat_ids[:, None] == jnp.arange(experts_all, dtype=jnp.int32)[None, :]).astype(
        jnp.int32
    )
    within = jnp.sum((jnp.cumsum(one_hot, axis=0) - 1) * one_hot, axis=1)
    slot_index = flat_ids * capacity + within
    row_of = jnp.arange(n_rows * per_row, dtype=jnp.int32) // per_row
    slot_owner = jnp.full((experts_all * capacity,), n_rows, jnp.int32).at[slot_index].set(row_of)
    return (slot_index.reshape(n_rows, per_row), slot_owner)


def mixer_half(queries, key_rows, value_rows, query_gain, key_gain, log_forget, out_weight):
    span_rows = queries.shape[0]
    heads_dev = queries.shape[1] // HEAD_SIZE
    kv_dev = key_rows.shape[1] // HEAD_SIZE
    group_ratio = heads_dev // kv_dev
    scale_qk = HEAD_SIZE ** (-0.5)
    q_normed = head_norm(
        queries.reshape(span_rows, kv_dev, group_ratio, HEAD_SIZE), query_gain
    ).astype(jnp.bfloat16)
    k_normed = head_norm(key_rows.reshape(span_rows, kv_dev, HEAD_SIZE), key_gain).astype(
        jnp.bfloat16
    )
    key_value = jnp.concatenate(
        [k_normed.reshape(span_rows, kv_dev * HEAD_SIZE), value_rows], axis=1
    )
    first_row = lax.axis_index("ep") * span_rows
    last_row = first_row + span_rows - 1
    query_pos = first_row + jnp.arange(span_rows, dtype=jnp.int32)
    query_gates = lax.dynamic_slice_in_dim(log_forget, first_row, span_rows, 1)
    query_gates = query_gates.T.reshape(span_rows, kv_dev, group_ratio)

    def add_block(running, kv_block, key_start):
        run_max, run_sum, run_acc = running
        block_len = kv_block.shape[0]
        k_block = kv_block[:, : kv_dev * HEAD_SIZE].reshape(block_len, kv_dev, HEAD_SIZE)
        v_block = kv_block[:, kv_dev * HEAD_SIZE :].reshape(block_len, kv_dev, HEAD_SIZE)
        key_gates = lax.dynamic_slice_in_dim(log_forget, key_start, block_len, 1)
        key_gates = key_gates.reshape(kv_dev, group_ratio, block_len)
        scores = (
            jnp.einsum("qgrd,kgd->qgrk", q_normed, k_block, preferred_element_type=jnp.float32)
            * scale_qk
        )
        scores = scores + query_gates[..., None] - key_gates[None]
        key_pos = key_start + jnp.arange(block_len, dtype=jnp.int32)
        visible = key_pos[None, :] <= query_pos[:, None]
        scores = jnp.where(visible[:, None, None, :], scores, -jnp.inf)
        new_max = jnp.maximum(run_max, jnp.max(scores, axis=-1))
        shrink = jnp.exp(run_max - new_max)
        weights = jnp.exp(scores - new_max[..., None])
        run_sum = shrink * run_sum + jnp.sum(weights, axis=-1)
        gathered = jnp.einsum(
            "qgrk,kgd->qgrd",
            weights.astype(jnp.bfloat16),
            v_block,
            preferred_element_type=jnp.float32,
        )
        return (new_max, run_sum, shrink[..., None] * run_acc + gathered)

    start_state = (
        jnp.full((span_rows, kv_dev, group_ratio), -jnp.inf, jnp.float32),
        jnp.zeros((span_rows, kv_dev, group_ratio), jnp.float32),
        jnp.zeros((span_rows, kv_dev, group_ratio, HEAD_SIZE), jnp.float32),
    )
    kv_piece = lax.all_gather(key_value, "ep", axis=0, tiled=True)
    block_len = min(kv_piece.shape[0], span_rows)
    n_blocks = kv_piece.shape[0] // block_len

    def one_block(block_number, running_in):
        key_start = block_number * block_len
        kv_block = lax.dynamic_slice_in_dim(kv_piece, block_number * block_len, block_len, 0)

        def take_block(running_now):
            return add_block(running_now, kv_block, key_start)

        def skip_block(running_now):
            return running_now

        return lax.cond(key_start <= last_row, take_block, skip_block, running_in)

    run_max, run_sum, run_acc = lax.fori_loop(0, n_blocks, one_block, start_state)
    attended = (
        (run_acc / run_sum[..., None])
        .astype(jnp.bfloat16)
        .reshape(span_rows, heads_dev * HEAD_SIZE)
    )
    return jnp.dot(attended, out_weight, preferred_element_type=jnp.float32).astype(jnp.bfloat16)


def experts_half(
    expert_rows, expert_gain, routes, route_weight, gate_weight, up_weight, down_weight
):
    n_tp = lax.axis_size("tp")
    n_ep = lax.axis_size("ep")
    span_rows = expert_rows.shape[0]
    model_width = expert_rows.shape[1]
    exp_dev = gate_weight.shape[0]
    capacity = n_tp * ((3 * (span_rows // n_tp) * TOP + 2 * EXPERTS - 1) // (2 * EXPERTS))
    normed = head_norm(expert_rows, expert_gain).astype(jnp.bfloat16)
    slot_index, slot_owner = slot_table(routes.T, EXPERTS, capacity)
    padded = jnp.concatenate([normed, jnp.zeros((1, model_width), jnp.bfloat16)], axis=0)
    part_len = capacity // n_tp
    owner_part = lax.dynamic_slice_in_dim(
        slot_owner.reshape(EXPERTS, capacity), lax.axis_index("tp") * part_len, part_len, 1
    )
    send_rows = padded[owner_part].reshape(n_ep, exp_dev, part_len, model_width)
    arrived = lax.all_to_all(send_rows, "ep", split_axis=0, concat_axis=0, tiled=True)
    slot_rows = lax.all_gather(arrived, "tp", axis=2, tiled=True)
    gate_part = jnp.einsum(
        "nxcd,xdf->nxcf", slot_rows, gate_weight, preferred_element_type=jnp.float32
    )
    up_part = jnp.einsum("nxcd,xdf->nxcf", slot_rows, up_weight, preferred_element_type=jnp.float32)
    hidden = (jax.nn.silu(gate_part) * up_part).astype(jnp.bfloat16)
    partial_out = jnp.einsum(
        "nxcf,xfd->nxcd", hidden, down_weight, preferred_element_type=jnp.float32
    )
    summed = lax.psum_scatter(
        partial_out.astype(jnp.bfloat16), "tp", scatter_dimension=3, tiled=True
    )
    returned = lax.all_to_all(summed, "ep", split_axis=0, concat_axis=0, tiled=True)
    result_table = returned.reshape(EXPERTS * capacity, returned.shape[3])
    picked = result_table[slot_index]
    combined = jnp.sum(picked.astype(jnp.float32) * route_weight.T[..., None], axis=1)
    return combined.astype(jnp.bfloat16)


LOG2E = 1.4426950408889634


def remote(src, dst, send_sem, recv_sem, peer):
    return pltpu.make_async_remote_copy(
        src_ref=src,
        dst_ref=dst,
        send_sem=send_sem,
        recv_sem=recv_sem,
        device_id=peer,
        device_id_type=pl.DeviceIdType.MESH,
    )


def dot_nt(lhs, rhs):
    return lax.dot_general(
        lhs, rhs, (((1,), (1,)), ((), ())), preferred_element_type=jnp.float32
    )


def dot_nn(lhs, rhs):
    return jnp.dot(lhs, rhs, preferred_element_type=jnp.float32)


def rows_of(index, size):
    return pl.ds(pl.multiple_of(index * size, size), size)


def one_hot(condition):
    return jnp.where(condition, 1.0, 0.0).astype(jnp.bfloat16)


def iota_f32(shape, dim):
    return lax.broadcasted_iota(jnp.int32, shape, dim).astype(jnp.float32)


def fused_kernel(
    n_ep,
    n_tp,
    capacity,
    q_hbm,
    k_hbm,
    v_hbm,
    qg_hbm,
    kg_hbm,
    lf_hbm,
    wo_hbm,
    x_hbm,
    xg_hbm,
    info_hbm,
    wg_hbm,
    wu_hbm,
    wd_hbm,
    mix_ref,
    exp_ref,
    q_in,
    k_in,
    kv,
    qg,
    kg,
    lf,
    wo,
    x_in,
    xg,
    info,
    wg,
    wu,
    wd,
    q_norm,
    run_max,
    run_sum,
    run_acc,
    att,
    mixp,
    mpaired,
    mleaving,
    mcrossed,
    normed,
    earlier,
    send_rows,
    arrived,
    gather_hot,
    return_hot,
    slot_weight,
    final_hot,
    slots,
    down,
    partial,
    paired,
    leaving,
    crossed,
    final,
    returned,
    in_sem,
    w_sem,
    kv_send,
    kv_recv,
    i_send,
    i_recv,
    z_send,
    z_recv,
    x_send,
    x_recv,
    c_send,
    c_recv,
    rc_send,
    rc_recv,
    rx_send,
    rx_recv,
    rz_send,
    rz_recv,
    m_send,
    m_recv,
):
    me = lax.axis_index("ep")
    mine = lax.axis_index("tp")
    pair = mine + 1 - 2 * (mine % 2)
    across = (mine + n_tp // 2) % n_tp
    pair_across = (pair + n_tp // 2) % n_tp
    span, width = x_in.shape
    heads = q_norm.shape[0]
    head = q_norm.shape[2]
    exp_dev = wg.shape[0]
    part = send_rows.shape[1]
    row_cap = part * n_tp
    n_slots = exp_dev * capacity
    quarter = width // n_tp
    score_scale = (head**-0.5) * LOG2E

    fetches = []

    def fetch(src, dst):
        copy = pltpu.make_async_copy(src, dst, in_sem.at[len(fetches)])
        copy.start()
        fetches.append(copy)
        return copy

    get_k = fetch(k_hbm, k_in)
    get_kg = fetch(kg_hbm, kg)
    get_v = fetch(v_hbm, kv.at[0, 1])
    get_info = fetch(info_hbm, info.at[0])
    get_x = fetch(x_hbm, x_in)
    get_xg = fetch(xg_hbm, xg)
    get_q = fetch(q_hbm, q_in)
    get_qg = fetch(qg_hbm, qg)
    get_lf = fetch(lf_hbm, lf)
    get_wo = fetch(wo_hbm, wo)
    weights = []
    for e in range(exp_dev):
        for i, (src, dst) in enumerate(((wg_hbm, wg), (wu_hbm, wu), (wd_hbm, wd))):
            copy = pltpu.make_async_copy(src.at[e], dst.at[e], w_sem.at[i, e])
            copy.start()
            weights.append(copy)

    barrier = pltpu.get_barrier_semaphore()
    peers = [{"ep": (me + k) % n_ep} for k in range(1, n_ep)] + [{"tp": pair}, {"tp": across}]
    for peer in peers:
        pl.semaphore_signal(barrier, inc=1, device_id=peer, device_id_type=pl.DeviceIdType.MESH)

    get_k.wait()
    get_kg.wait()

    def norm_heads(rows, gain):
        factor = lax.rsqrt(jnp.mean(rows * rows, axis=-1, keepdims=True) + 1e-06)
        return (rows * factor * gain).astype(jnp.bfloat16)

    kv[0, 0] = norm_heads(k_in[...].astype(jnp.float32), kg[...])
    get_info.wait()
    get_v.wait()
    pl.semaphore_wait(barrier, len(peers))

    notes_sent = []
    for k in range(1, n_ep):
        copy = remote(
            info_hbm, info.at[k], i_send.at[k], i_recv.at[k], {"ep": (me + k) % n_ep}
        )
        copy.start()
        notes_sent.append(copy)

    kv_copies = [
        remote(kv.at[d], kv.at[d + 1], kv_send.at[d], kv_recv.at[d + 1], {"ep": (me + 1) % n_ep})
        for d in range(n_ep - 1)
    ]

    def kv_pass(d):
        @pl.when((me >= d) & (me < n_ep - 1))
        def _():
            kv_copies[d].start()

    kv_pass(0)

    me_f = me.astype(jnp.float32)
    earlier[...] = one_hot(iota_f32((span, span), 0) < iota_f32((span, span), 1))
    kinds = iota_f32((8, span), 0)

    def ranks(k):
        table = info[k]
        dest = table[0:1]
        at_me = dest == me_f
        local = [jnp.where(at_me, table[1 + j : 2 + j], -1.0) for j in range(TOP)]
        to_dest = jnp.where(dest == kinds, 1.0, 0.0)
        picks = [jnp.where(local[j] == kinds, 1.0, 0.0) for j in range(TOP)]
        marks = jnp.concatenate([to_dest, picks[0] + picks[1]], axis=0).astype(jnp.bfloat16)
        ahead = dot_nn(marks, earlier[...])
        rank = jnp.sum(to_dest * ahead[:8], axis=0, keepdims=True)
        within = [jnp.sum(picks[j] * ahead[8:], axis=0, keepdims=True) for j in range(TOP)]
        return table, dest, at_me, local, rank, within

    def slot_tables(k, ranked):
        table, dest, at_me, local, rank, within = ranked
        row_key = jnp.where(at_me, rank, -1.0)
        picked = one_hot(iota_f32((row_cap, span), 0) == row_key)
        columns = jnp.zeros((8, span), jnp.float32)
        entries = [local[0] + 1.0, within[0], local[1] + 1.0, within[1]]
        entries += [table[3 + i : 4 + i] for i in range(4)]
        for i, entry in enumerate(entries):
            columns = jnp.where(kinds == float(i), entry, columns)
        columns = jnp.concatenate([columns, jnp.zeros((8, span), jnp.float32)], axis=0)
        columns = columns.astype(jnp.bfloat16)
        across_rows = dot_nt(columns, picked)
        along_rows = dot_nt(picked, columns)
        slot_ids = iota_f32((n_slots, row_cap), 0)
        slot_lanes = iota_f32((row_cap, n_slots), 1)
        lane_hits = []
        gains = 0.0
        hot = 0.0
        for j in range(TOP):
            level = across_rows[2 * j : 2 * j + 1]
            slot = jnp.where(
                level > 0.5, (level - 1.0) * capacity + across_rows[2 * j + 1 : 2 * j + 2], -1.0
            )
            weight = across_rows[4 + 2 * j : 5 + 2 * j] + across_rows[5 + 2 * j : 6 + 2 * j]
            match = slot_ids == slot
            hot = hot + jnp.where(match, 1.0, 0.0)
            gains = gains + jnp.where(match, weight, 0.0)
            level = along_rows[:, 2 * j : 2 * j + 1]
            slot = jnp.where(
                level > 0.5, (level - 1.0) * capacity + along_rows[:, 2 * j + 1 : 2 * j + 2], -1.0
            )
            lane_hits.append(jnp.where(slot_lanes == slot, 1.0, 0.0))
        gather_hot[k] = hot.astype(jnp.bfloat16)
        return_hot[k] = (lane_hits[0] + lane_hits[1]).astype(jnp.bfloat16)
        slot_weight[k] = jnp.sum(gains, axis=1, keepdims=True)

    get_x.wait()
    get_xg.wait()
    norm_rows = 32

    def norm_tile(i, carry):
        rows = rows_of(i, norm_rows)
        normed[rows, :] = norm_heads(x_in[rows, :].astype(jnp.float32), xg[...])
        return carry

    lax.fori_loop(0, span // norm_rows, norm_tile, 0)
    own = ranks(0)
    _, dest, _, _, rank, _ = own
    token_key = dest * row_cap + rank
    part_base = (mine * part).astype(jnp.float32)
    part_rows = iota_f32((part, span), 0) + part_base
    chosen = []
    for k in range(1, n_ep):
        base = ((me + k) % n_ep * row_cap).astype(jnp.float32)
        chosen.append(jnp.where(part_rows + base == token_key, 1.0, 0.0))
    chosen = jnp.concatenate(chosen, axis=0).astype(jnp.bfloat16)
    col = 256

    def send_tile(i, carry):
        cols = rows_of(i, col)
        rows = dot_nn(chosen, normed[:, cols]).astype(jnp.bfloat16)
        for k in range(1, n_ep):
            send_rows[k - 1, :, cols] = rows[(k - 1) * part : k * part]
        return carry

    lax.fori_loop(0, width // col, send_tile, 0)
    along = {}
    for k in range(1, n_ep):
        copy = remote(
            send_rows.at[k - 1],
            arrived.at[k, mine],
            z_send.at[k],
            z_recv.at[k],
            {"ep": (me + k) % n_ep},
        )
        copy.start()
        along[k] = copy

    own_rows = one_hot(
        iota_f32((row_cap, span), 0) + (me * row_cap).astype(jnp.float32) == token_key
    )

    def own_tile(i, carry):
        cols = rows_of(i, col)
        rows = dot_nn(own_rows, normed[:, cols]).astype(jnp.bfloat16)
        for p in range(n_tp):
            arrived[0, p, :, cols] = rows[p * part : (p + 1) * part]
        return carry

    lax.fori_loop(0, width // col, own_tile, 0)

    get_q.wait()
    get_qg.wait()
    get_lf.wait()
    for h in range(heads):
        q_norm[h] = norm_heads(
            q_in[:, h * head : (h + 1) * head].astype(jnp.float32), qg[...]
        )
    tile = 256
    first_token = pl.multiple_of(me * span, span)

    def attend(d):
        key_start = pl.multiple_of((me - d) * span, span)
        for h in range(heads):
            start_gate = lf[h : h + 1, pl.ds(first_token, head)][:, 0:1]
            gate = (start_gate - lf[h : h + 1, pl.ds(key_start, span)]) * LOG2E

            def query_tile(i, carry):
                rows = rows_of(i, tile)
                scores = dot_nt(q_norm[h, rows, :], kv[d, 0]) * score_scale + gate
                if d == 0:
                    key_at = lax.broadcasted_iota(jnp.int32, (tile, span), 1)
                    query_at = lax.broadcasted_iota(jnp.int32, (tile, span), 0) + i * tile
                    scores = jnp.where(key_at <= query_at, scores, -jnp.inf)
                top = jnp.max(scores, axis=-1, keepdims=True)
                if d == 0:
                    prob = jnp.exp2(scores - top)
                    run_max[h, rows, :] = top
                    run_sum[h, rows, :] = jnp.sum(prob, axis=-1, keepdims=True)
                    run_acc[h, rows, :] = dot_nn(prob.astype(jnp.bfloat16), kv[d, 1])
                else:
                    old = run_max[h, rows, :]
                    top = jnp.maximum(old, top)
                    shrink = jnp.exp2(old - top)
                    prob = jnp.exp2(scores - top)
                    run_max[h, rows, :] = top
                    run_sum[h, rows, :] = run_sum[h, rows, :] * shrink + jnp.sum(
                        prob, axis=-1, keepdims=True
                    )
                    run_acc[h, rows, :] = run_acc[h, rows, :] * shrink + dot_nn(
                        prob.astype(jnp.bfloat16), kv[d, 1]
                    )
                return carry

            lax.fori_loop(0, span // tile, query_tile, 0)

    attend(0)

    def kv_step(d):
        @pl.when(me >= d)
        def _():
            kv_copies[d - 1].wait_recv()

        if d < n_ep - 1:
            kv_pass(d)

        @pl.when(me >= d)
        def _():
            attend(d)

    crossing = {}
    pairing = {}

    def pass_on(k):
        along[k].wait_recv()
        place = arrived.at[k, mine]
        copy = remote(place, place, x_send.at[k], x_recv.at[k], {"tp": across})
        copy.start()
        crossing[k] = copy
        copy = remote(place, place, c_send.at[0, k], c_recv.at[0, k], {"tp": pair})
        copy.start()
        pairing[0, k] = copy

    def relay(k):
        crossing[k].wait_recv()
        place = arrived.at[k, across]
        copy = remote(place, place, c_send.at[1, k], c_recv.at[1, k], {"tp": pair})
        copy.start()
        pairing[1, k] = copy

    def fill_slots(k, side):
        if k > 0:
            pairing[0, k].wait_recv()
            pairing[1, k].wait_recv()

        def slot_tile(i, carry):
            cols = rows_of(i, col)
            rows = arrived[k, :, :, cols].reshape(row_cap, col)
            filled = dot_nn(gather_hot[k], rows).astype(jnp.bfloat16)
            for e in range(exp_dev):
                slots[e, side * capacity : (side + 1) * capacity, cols] = filled[
                    e * capacity : (e + 1) * capacity
                ]
            return carry

        lax.fori_loop(0, width // col, slot_tile, 0)

    wide = 512

    def expert_pass(sources):
        def one_expert(e, carry):
            rows = slots[e]
            gate_part = dot_nn(rows, wg[e])
            up_part = dot_nn(rows, wu[e])
            weight = jnp.concatenate(
                [slot_weight[k, rows_of(e, capacity), :] for k in sources], axis=0
            )
            hidden = gate_part / (1.0 + jnp.exp(-gate_part)) * up_part * weight
            hidden = hidden.astype(jnp.bfloat16)
            for c in range(width // wide):
                cols = slice(c * wide, (c + 1) * wide)
                result = dot_nn(hidden, wd[e, :, cols]).astype(jnp.bfloat16)
                for side in range(len(sources)):
                    down[side, e, :, cols] = result[side * capacity : (side + 1) * capacity]
            return carry

        lax.fori_loop(0, exp_dev, one_expert, 0)

    back_pairing = {}
    back_crossing = {}
    back_along = {}
    order = list(range(1, n_ep)) + [0]

    def combine(k, side):
        def combine_tile(c, carry):
            cols = rows_of(c, quarter)
            rows = down[side, :, :, cols].reshape(n_slots, quarter)
            partial[k, c] = dot_nn(return_hot[k], rows).astype(jnp.bfloat16)
            return carry

        lax.fori_loop(0, n_tp, combine_tile, 0)
        for way, block in ((1, pair_across), (0, pair)):
            copy = remote(
                partial.at[k, block],
                paired.at[way, k],
                rc_send.at[way, k],
                rc_recv.at[way, k],
                {"tp": pair},
            )
            copy.start()
            back_pairing[way, k] = copy

    def back_cross(k):
        back_pairing[1, k].wait_recv()
        leaving[k] = (
            partial[k, across].astype(jnp.float32) + paired[1, k].astype(jnp.float32)
        ).astype(jnp.bfloat16)
        copy = remote(leaving.at[k], crossed.at[k], rx_send.at[k], rx_recv.at[k], {"tp": across})
        copy.start()
        back_crossing[k] = copy

    def back_send(k):
        back_pairing[0, k].wait_recv()
        back_crossing[k].wait_recv()
        total = partial[k, mine].astype(jnp.float32) + paired[0, k].astype(jnp.float32)
        total = (total + crossed[k].astype(jnp.float32)).astype(jnp.bfloat16)
        if k == 0:
            returned[0] = total
            return
        final[k] = total
        source = (me + n_ep - k) % n_ep
        copy = remote(final.at[k], returned.at[k], rz_send.at[k], rz_recv.at[k], {"ep": source})
        copy.start()
        back_along[k] = copy

    mixer = {}

    def mixer_start():
        get_wo.wait()
        for h in range(heads):
            att[:, h * head : (h + 1) * head] = (run_acc[h] / run_sum[h]).astype(jnp.bfloat16)

        def project(c, carry):
            cols = rows_of(c, col)
            rows = dot_nn(att[...], wo[:, cols]).astype(jnp.bfloat16)
            mixp[:, :, cols] = rows.reshape(n_tp, span // n_tp, col)
            return carry

        lax.fori_loop(0, width // col, project, 0)
        for way, block in ((1, pair_across), (0, pair)):
            copy = remote(
                mixp.at[block], mpaired.at[way], m_send.at[way], m_recv.at[way], {"tp": pair}
            )
            copy.start()
            mixer[way] = copy

    step = 16

    def mixer_cross():
        mixer[1].wait_recv()

        def add_tile(i, carry):
            rows = rows_of(i, step)
            mleaving[rows, :] = (
                mixp[across, rows, :].astype(jnp.float32) + mpaired[1, rows, :].astype(jnp.float32)
            ).astype(jnp.bfloat16)
            return carry

        lax.fori_loop(0, span // n_tp // step, add_tile, 0)
        copy = remote(mleaving, mcrossed, m_send.at[2], m_recv.at[2], {"tp": across})
        copy.start()
        mixer[2] = copy

    def mixer_end():
        mixer[0].wait_recv()
        mixer[2].wait_recv()

        def add_tile(i, carry):
            rows = rows_of(i, step)
            total = mixp[mine, rows, :].astype(jnp.float32) + mpaired[0, rows, :].astype(
                jnp.float32
            )
            mix_ref[rows, :] = (total + mcrossed[rows, :].astype(jnp.float32)).astype(
                jnp.bfloat16
            )
            return carry

        lax.fori_loop(0, span // n_tp // step, add_tile, 0)

    slot_tables(0, own)
    fill_slots(0, 0)
    token_column = jnp.transpose(jnp.broadcast_to(token_key, (8, span)), (1, 0))[:, 0:1]
    for k in range(n_ep):
        base = ((me + k) % n_ep * row_cap).astype(jnp.float32)
        final_hot[:, k * row_cap : (k + 1) * row_cap] = one_hot(
            iota_f32((span, row_cap), 1) + base == token_column
        )
    for k in range(1, n_ep):
        notes_sent[k - 1].wait_recv()
        slot_tables(k, ranks(k))
    pass_on(1)
    kv_step(1)
    relay(1)
    for copy in weights:
        copy.wait()
    fill_slots(1, 1)
    expert_pass((0, 1))
    combine(1, 1)
    combine(0, 0)
    pass_on(2)
    back_cross(1)
    back_cross(0)
    relay(2)
    pass_on(3)
    kv_step(2)
    back_send(1)
    back_send(0)
    relay(3)
    fill_slots(2, 0)
    fill_slots(3, 1)
    expert_pass((2, 3))
    combine(2, 0)
    combine(3, 1)
    back_cross(2)
    back_cross(3)
    kv_step(3)
    mixer_start()
    back_send(2)
    mixer_cross()
    back_send(3)
    for k in range(1, n_ep):
        back_along[k].wait_recv()

    def output_tile(i, carry):
        rows = rows_of(i, 128)
        exp_ref[rows, :] = dot_nn(
            final_hot[rows, :], returned[...].reshape(n_ep * row_cap, quarter)
        ).astype(jnp.bfloat16)
        return carry

    lax.fori_loop(0, span // 128, output_tile, 0)
    mixer_end()

    for copy in notes_sent:
        copy.wait_send()
    for d in range(n_ep - 1):

        @pl.when((me >= d) & (me < n_ep - 1))
        def _():
            kv_copies[d].wait_send()

    for group in (along, crossing, pairing, back_pairing, back_crossing, back_along, mixer):
        for copy in group.values():
            copy.wait_send()


def fused_half(
    queries,
    key_rows,
    value_rows,
    query_gain,
    key_gain,
    log_forget,
    out_weight,
    expert_rows,
    expert_gain,
    routes,
    route_weight,
    gate_weight,
    up_weight,
    down_weight,
    capacity,
):
    n_tp = lax.axis_size("tp")
    n_ep = lax.axis_size("ep")
    span, width = expert_rows.shape
    exp_dev = gate_weight.shape[0]
    hidden = gate_weight.shape[2]
    heads = queries.shape[1] // HEAD_SIZE
    row_cap = exp_dev * capacity // TOP
    part = row_cap // n_tp
    quarter = width // n_tp
    n_slots = exp_dev * capacity
    whole = log_forget.shape[1]
    weight_rows = []
    for j in range(TOP):
        high = lax.reduce_precision(route_weight[j], 8, 7)
        weight_rows += [high, route_weight[j] - high]
    info = jnp.stack(
        [(routes[0] // exp_dev).astype(jnp.float32)]
        + [(routes[j] % exp_dev).astype(jnp.float32) for j in range(TOP)]
        + weight_rows
        + [jnp.zeros((span,), jnp.float32)],
        axis=0,
    )
    low = jnp.bfloat16
    full = jnp.float32
    vmem = pltpu.VMEM
    dma = pltpu.SemaphoreType.DMA
    scratch = [
        vmem((span, heads * HEAD_SIZE), low),
        vmem((span, HEAD_SIZE), low),
        vmem((n_ep, 2, span, HEAD_SIZE), low),
        vmem((1, HEAD_SIZE), full),
        vmem((1, HEAD_SIZE), full),
        vmem((heads, whole), full),
        vmem((heads * HEAD_SIZE, width), low),
        vmem((span, width), low),
        vmem((1, width), full),
        vmem((n_ep, 8, span), full),
        vmem((exp_dev, width, hidden), low),
        vmem((exp_dev, width, hidden), low),
        vmem((exp_dev, hidden, width), low),
        vmem((heads, span, HEAD_SIZE), low),
        vmem((heads, span, 1), full),
        vmem((heads, span, 1), full),
        vmem((heads, span, HEAD_SIZE), full),
        vmem((span, heads * HEAD_SIZE), low),
        vmem((n_tp, span // n_tp, width), low),
        vmem((2, span // n_tp, width), low),
        vmem((span // n_tp, width), low),
        vmem((span // n_tp, width), low),
        vmem((span, width), low),
        vmem((span, span), low),
        vmem((n_ep - 1, part, width), low),
        vmem((n_ep, n_tp, part, width), low),
        vmem((n_ep, n_slots, row_cap), low),
        vmem((n_ep, row_cap, n_slots), low),
        vmem((n_ep, n_slots, 1), full),
        vmem((span, n_ep * row_cap), low),
        vmem((exp_dev, 2 * capacity, width), low),
        vmem((2, exp_dev, capacity, width), low),
        vmem((n_ep, n_tp, row_cap, quarter), low),
        vmem((2, n_ep, row_cap, quarter), low),
        vmem((n_ep, row_cap, quarter), low),
        vmem((n_ep, row_cap, quarter), low),
        vmem((n_ep, row_cap, quarter), low),
        vmem((n_ep, row_cap, quarter), low),
        dma((10,)),
        dma((3, exp_dev)),
        dma((n_ep,)),
        dma((n_ep,)),
        dma((n_ep,)),
        dma((n_ep,)),
        dma((n_ep,)),
        dma((n_ep,)),
        dma((n_ep,)),
        dma((n_ep,)),
        dma((2, n_ep)),
        dma((2, n_ep)),
        dma((2, n_ep)),
        dma((2, n_ep)),
        dma((n_ep,)),
        dma((n_ep,)),
        dma((n_ep,)),
        dma((n_ep,)),
        dma((3,)),
        dma((3,)),
    ]
    return pl.pallas_call(
        functools.partial(fused_kernel, n_ep, n_tp, capacity),
        out_shape=(
            jax.ShapeDtypeStruct((span // n_tp, width), low),
            jax.ShapeDtypeStruct((span, quarter), low),
        ),
        in_specs=[pl.BlockSpec(memory_space=pl.ANY)] * 13,
        out_specs=(
            pl.BlockSpec(memory_space=pltpu.VMEM),
            pl.BlockSpec(memory_space=pltpu.VMEM),
        ),
        scratch_shapes=scratch,
        compiler_params=pltpu.CompilerParams(
            collective_id=0, has_side_effects=True, vmem_limit_bytes=VMEM_LIMIT
        ),
    )(
        queries,
        key_rows,
        value_rows,
        query_gain.reshape(1, -1),
        key_gain.reshape(1, -1),
        log_forget,
        out_weight,
        expert_rows,
        expert_gain.reshape(1, -1),
        info,
        gate_weight,
        up_weight,
        down_weight,
    )


def on_device(
    queries,
    key_rows,
    value_rows,
    query_gain,
    key_gain,
    log_forget,
    out_weight,
    expert_rows,
    expert_gain,
    routes,
    route_weight,
    gate_weight,
    up_weight,
    down_weight,
):
    mixer_args = (
        queries,
        key_rows,
        value_rows,
        query_gain,
        key_gain,
        log_forget,
        out_weight,
    )
    expert_args = (
        expert_rows,
        expert_gain,
        routes,
        route_weight,
        gate_weight,
        up_weight,
        down_weight,
    )
    n_tp = lax.axis_size("tp")
    n_ep = lax.axis_size("ep")
    span = expert_rows.shape[0]
    capacity = n_tp * ((3 * (span // n_tp) * TOP + 2 * EXPERTS - 1) // (2 * EXPERTS))
    fits = (
        n_tp == 4
        and n_ep == 4
        and gate_weight.shape[0] == GROUP_SIZE
        and capacity % 16 == 0
        and key_rows.shape[1] == HEAD_SIZE
    )
    if fits:
        return fused_half(*mixer_args, *expert_args, capacity)
    expert_out = experts_half(*expert_args)
    mixer_part = mixer_half(*mixer_args)
    mixer_out = lax.psum_scatter(mixer_part, "tp", scatter_dimension=0, tiled=True)
    return (mixer_out, expert_out)


def solution(mesh):
    in_specs = (
        P(("grp", "ep"), "tp"),
        P(("grp", "ep"), "tp"),
        P(("grp", "ep"), "tp"),
        P(),
        P(),
        P("tp", "grp"),
        P("tp", None),
        P(("grp", "ep"), None),
        P(),
        P(None, ("grp", "ep")),
        P(None, ("grp", "ep")),
        P("ep", None, "tp"),
        P("ep", None, "tp"),
        P("ep", "tp", None),
    )
    out_specs = (P(("grp", "ep", "tp"), None), P(("grp", "ep"), "tp"))
    return jax.shard_map(
        on_device, mesh=mesh, in_specs=in_specs, out_specs=out_specs, check_vma=False
    )
```

```python
import functools

import jax
import jax.numpy as jnp
from jax import lax
from jax.experimental import pallas as pl
from jax.experimental.pallas import tpu as pltpu
from jax.sharding import PartitionSpec as P

HEAD_SIZE = 128
EXPERTS = 32
TOP = 2
GROUP_SIZE = 8
VMEM_LIMIT = 65000 * 1024
PIECES = 2


def head_norm(inputs, scale_gain):
    widened = inputs.astype(jnp.float32)
    factor = lax.rsqrt(jnp.mean(widened * widened, axis=-1, keepdims=True) + 1e-06)
    return widened * factor * scale_gain


def slot_table(chosen, experts_all, capacity):
    n_rows = chosen.shape[0]
    per_row = chosen.shape[1]
    flat_ids = chosen.reshape(-1)
    one_hot = (flat_ids[:, None] == jnp.arange(experts_all, dtype=jnp.int32)[None, :]).astype(
        jnp.int32
    )
    within = jnp.sum((jnp.cumsum(one_hot, axis=0) - 1) * one_hot, axis=1)
    slot_index = flat_ids * capacity + within
    row_of = jnp.arange(n_rows * per_row, dtype=jnp.int32) // per_row
    slot_owner = jnp.full((experts_all * capacity,), n_rows, jnp.int32).at[slot_index].set(row_of)
    return (slot_index.reshape(n_rows, per_row), slot_owner)


def mixer_half(queries, key_rows, value_rows, query_gain, key_gain, log_forget, out_weight):
    span_rows = queries.shape[0]
    heads_dev = queries.shape[1] // HEAD_SIZE
    kv_dev = key_rows.shape[1] // HEAD_SIZE
    group_ratio = heads_dev // kv_dev
    scale_qk = HEAD_SIZE ** (-0.5)
    q_normed = head_norm(
        queries.reshape(span_rows, kv_dev, group_ratio, HEAD_SIZE), query_gain
    ).astype(jnp.bfloat16)
    k_normed = head_norm(key_rows.reshape(span_rows, kv_dev, HEAD_SIZE), key_gain).astype(
        jnp.bfloat16
    )
    key_value = jnp.concatenate(
        [k_normed.reshape(span_rows, kv_dev * HEAD_SIZE), value_rows], axis=1
    )
    first_row = lax.axis_index("ep") * span_rows
    last_row = first_row + span_rows - 1
    query_pos = first_row + jnp.arange(span_rows, dtype=jnp.int32)
    query_gates = lax.dynamic_slice_in_dim(log_forget, first_row, span_rows, 1)
    query_gates = query_gates.T.reshape(span_rows, kv_dev, group_ratio)

    def add_block(running, kv_block, key_start):
        run_max, run_sum, run_acc = running
        block_len = kv_block.shape[0]
        k_block = kv_block[:, : kv_dev * HEAD_SIZE].reshape(block_len, kv_dev, HEAD_SIZE)
        v_block = kv_block[:, kv_dev * HEAD_SIZE :].reshape(block_len, kv_dev, HEAD_SIZE)
        key_gates = lax.dynamic_slice_in_dim(log_forget, key_start, block_len, 1)
        key_gates = key_gates.reshape(kv_dev, group_ratio, block_len)
        scores = (
            jnp.einsum("qgrd,kgd->qgrk", q_normed, k_block, preferred_element_type=jnp.float32)
            * scale_qk
        )
        scores = scores + query_gates[..., None] - key_gates[None]
        key_pos = key_start + jnp.arange(block_len, dtype=jnp.int32)
        visible = key_pos[None, :] <= query_pos[:, None]
        scores = jnp.where(visible[:, None, None, :], scores, -jnp.inf)
        new_max = jnp.maximum(run_max, jnp.max(scores, axis=-1))
        shrink = jnp.exp(run_max - new_max)
        weights = jnp.exp(scores - new_max[..., None])
        run_sum = shrink * run_sum + jnp.sum(weights, axis=-1)
        gathered = jnp.einsum(
            "qgrk,kgd->qgrd",
            weights.astype(jnp.bfloat16),
            v_block,
            preferred_element_type=jnp.float32,
        )
        return (new_max, run_sum, shrink[..., None] * run_acc + gathered)

    start_state = (
        jnp.full((span_rows, kv_dev, group_ratio), -jnp.inf, jnp.float32),
        jnp.zeros((span_rows, kv_dev, group_ratio), jnp.float32),
        jnp.zeros((span_rows, kv_dev, group_ratio, HEAD_SIZE), jnp.float32),
    )
    kv_piece = lax.all_gather(key_value, "ep", axis=0, tiled=True)
    block_len = min(kv_piece.shape[0], span_rows)
    n_blocks = kv_piece.shape[0] // block_len

    def one_block(block_number, running_in):
        key_start = block_number * block_len
        kv_block = lax.dynamic_slice_in_dim(kv_piece, block_number * block_len, block_len, 0)

        def take_block(running_now):
            return add_block(running_now, kv_block, key_start)

        def skip_block(running_now):
            return running_now

        return lax.cond(key_start <= last_row, take_block, skip_block, running_in)

    run_max, run_sum, run_acc = lax.fori_loop(0, n_blocks, one_block, start_state)
    attended = (
        (run_acc / run_sum[..., None])
        .astype(jnp.bfloat16)
        .reshape(span_rows, heads_dev * HEAD_SIZE)
    )
    return jnp.dot(attended, out_weight, preferred_element_type=jnp.float32).astype(jnp.bfloat16)


def experts_half(
    expert_rows, expert_gain, routes, route_weight, gate_weight, up_weight, down_weight
):
    n_tp = lax.axis_size("tp")
    n_ep = lax.axis_size("ep")
    span_rows = expert_rows.shape[0]
    model_width = expert_rows.shape[1]
    exp_dev = gate_weight.shape[0]
    capacity = n_tp * ((3 * (span_rows // n_tp) * TOP + 2 * EXPERTS - 1) // (2 * EXPERTS))
    normed = head_norm(expert_rows, expert_gain).astype(jnp.bfloat16)
    slot_index, slot_owner = slot_table(routes.T, EXPERTS, capacity)
    padded = jnp.concatenate([normed, jnp.zeros((1, model_width), jnp.bfloat16)], axis=0)
    part_len = capacity // n_tp
    owner_part = lax.dynamic_slice_in_dim(
        slot_owner.reshape(EXPERTS, capacity), lax.axis_index("tp") * part_len, part_len, 1
    )
    send_rows = padded[owner_part].reshape(n_ep, exp_dev, part_len, model_width)
    arrived = lax.all_to_all(send_rows, "ep", split_axis=0, concat_axis=0, tiled=True)
    slot_rows = lax.all_gather(arrived, "tp", axis=2, tiled=True)
    gate_part = jnp.einsum(
        "nxcd,xdf->nxcf", slot_rows, gate_weight, preferred_element_type=jnp.float32
    )
    up_part = jnp.einsum("nxcd,xdf->nxcf", slot_rows, up_weight, preferred_element_type=jnp.float32)
    hidden = (jax.nn.silu(gate_part) * up_part).astype(jnp.bfloat16)
    partial_out = jnp.einsum(
        "nxcf,xfd->nxcd", hidden, down_weight, preferred_element_type=jnp.float32
    )
    summed = lax.psum_scatter(
        partial_out.astype(jnp.bfloat16), "tp", scatter_dimension=3, tiled=True
    )
    returned = lax.all_to_all(summed, "ep", split_axis=0, concat_axis=0, tiled=True)
    result_table = returned.reshape(EXPERTS * capacity, returned.shape[3])
    picked = result_table[slot_index]
    combined = jnp.sum(picked.astype(jnp.float32) * route_weight.T[..., None], axis=1)
    return combined.astype(jnp.bfloat16)


LOG2E = 1.4426950408889634


def remote(src, dst, send_sem, recv_sem, peer):
    return pltpu.make_async_remote_copy(
        src_ref=src,
        dst_ref=dst,
        send_sem=send_sem,
        recv_sem=recv_sem,
        device_id=peer,
        device_id_type=pl.DeviceIdType.MESH,
    )


def dot_nt(lhs, rhs):
    return lax.dot_general(
        lhs, rhs, (((1,), (1,)), ((), ())), preferred_element_type=jnp.float32
    )


def dot_nn(lhs, rhs):
    return jnp.dot(lhs, rhs, preferred_element_type=jnp.float32)


def rows_of(index, size):
    return pl.ds(pl.multiple_of(index * size, size), size)


def one_hot(condition):
    return jnp.where(condition, 1.0, 0.0).astype(jnp.bfloat16)


def iota_f32(shape, dim):
    return lax.broadcasted_iota(jnp.int32, shape, dim).astype(jnp.float32)


def fused_kernel(
    n_ep,
    n_tp,
    capacity,
    q_hbm,
    k_hbm,
    v_hbm,
    qg_hbm,
    kg_hbm,
    lf_hbm,
    wo_hbm,
    x_hbm,
    xg_hbm,
    routes_hbm,
    share_hbm,
    wg_hbm,
    wu_hbm,
    wd_hbm,
    mix_ref,
    exp_ref,
    q_in,
    k_in,
    kv,
    qg,
    kg,
    lf,
    wo,
    x_in,
    xg,
    routes,
    share,
    info,
    wg,
    wu,
    wd,
    q_norm,
    run_max,
    run_sum,
    run_acc,
    att,
    mixp,
    mpaired,
    mleaving,
    mcrossed,
    normed,
    earlier,
    send_rows,
    arrived,
    gather_hot,
    return_hot,
    slot_weight,
    final_hot,
    exp_acc,
    slots,
    down,
    partial,
    paired,
    leaving,
    crossed,
    final,
    returned,
    in_sem,
    w_sem,
    kv_send,
    kv_recv,
    i_send,
    i_recv,
    z_send,
    z_recv,
    x_send,
    x_recv,
    c_send,
    c_recv,
    rc_send,
    rc_recv,
    rx_send,
    rx_recv,
    rz_send,
    rz_recv,
    m_send,
    m_recv,
):
    me = lax.axis_index("ep")
    mine = lax.axis_index("tp")
    pair = mine + 1 - 2 * (mine % 2)
    across = (mine + n_tp // 2) % n_tp
    pair_across = (pair + n_tp // 2) % n_tp
    span, width = x_in.shape
    heads = q_norm.shape[0]
    head = q_norm.shape[2]
    exp_dev = wg.shape[0]
    part = send_rows.shape[1]
    row_cap = part * n_tp
    n_slots = exp_dev * capacity
    quarter = width // n_tp
    score_scale = (head**-0.5) * LOG2E
    near = n_ep - 1 - (n_ep - 2) * (me // (n_ep - 1))
    middle = 2 - me * (n_ep - 1 - me) // 2
    order = (near, middle, 2 * n_ep - 2 - near - middle)

    fetches = []

    def fetch(src, dst):
        copy = pltpu.make_async_copy(src, dst, in_sem.at[len(fetches)])
        copy.start()
        fetches.append(copy)
        return copy

    get_k = fetch(k_hbm, k_in)
    get_kg = fetch(kg_hbm, kg)
    get_v = fetch(v_hbm, kv.at[0, 1])
    get_routes = fetch(routes_hbm, routes)
    get_share = fetch(share_hbm, share)
    get_x = fetch(x_hbm, x_in)
    get_xg = fetch(xg_hbm, xg)
    get_q = fetch(q_hbm, q_in)
    get_qg = fetch(qg_hbm, qg)
    get_lf = fetch(lf_hbm, lf)
    get_wo = fetch(wo_hbm, wo)
    barrier = pltpu.get_barrier_semaphore()
    peers = [{"ep": (me + k) % n_ep} for k in range(1, n_ep)] + [{"tp": pair}, {"tp": across}]
    for peer in peers:
        pl.semaphore_signal(barrier, inc=1, device_id=peer, device_id_type=pl.DeviceIdType.MESH)

    get_k.wait()
    get_kg.wait()

    def norm_heads(rows, gain):
        factor = lax.rsqrt(jnp.mean(rows * rows, axis=-1, keepdims=True) + 1e-06)
        return (rows * factor * gain).astype(jnp.bfloat16)

    kv[0, 0] = norm_heads(k_in[...].astype(jnp.float32), kg[...])
    get_routes.wait()
    get_share.wait()
    get_v.wait()
    chosen_ids = routes[...].astype(jnp.float32)
    shares = share[...]
    high = shares.astype(jnp.bfloat16).astype(jnp.float32)
    group = jnp.zeros((1, span), jnp.float32)
    for d in range(1, n_ep):
        group = group + jnp.where(chosen_ids[0:1] >= float(d * exp_dev), 1.0, 0.0)
    kinds = iota_f32((8, span), 0)
    entries = [group] + [chosen_ids[j : j + 1] - group * exp_dev for j in range(TOP)]
    for j in range(TOP):
        entries += [high[j : j + 1], shares[j : j + 1] - high[j : j + 1]]
    table = jnp.zeros((8, span), jnp.float32)
    for i, entry in enumerate(entries):
        table = jnp.where(kinds == float(i), entry, table)
    info[0] = table
    pl.semaphore_wait(barrier, len(peers))

    kv_copies = [
        [
            remote(
                kv.at[d, i],
                kv.at[d + 1, i],
                kv_send.at[d, i],
                kv_recv.at[d + 1, i],
                {"ep": (me + 1) % n_ep},
            )
            for i in range(2)
        ]
        for d in range(n_ep - 1)
    ]

    def kv_pass(d, i):
        @pl.when((me >= d) & (me < n_ep - 1))
        def _():
            kv_copies[d][i].start()

    kv_pass(0, 0)

    @pl.when(me == 0)
    def _():
        kv_copies[0][1].start()

    notes_sent = []
    for k in range(1, n_ep):
        copy = remote(
            info.at[0], info.at[k], i_send.at[k], i_recv.at[k], {"ep": (me + k) % n_ep}
        )
        copy.start()
        notes_sent.append(copy)

    me_f = me.astype(jnp.float32)
    earlier[...] = one_hot(iota_f32((span, span), 0) < iota_f32((span, span), 1))

    def ranks(k):
        table = info[k]
        dest = table[0:1]
        at_me = dest == me_f
        local = [jnp.where(at_me, table[1 + j : 2 + j], -1.0) for j in range(TOP)]
        to_dest = jnp.where(dest == kinds, 1.0, 0.0)
        picks = [jnp.where(local[j] == kinds, 1.0, 0.0) for j in range(TOP)]
        marks = jnp.concatenate([to_dest, picks[0] + picks[1]], axis=0).astype(jnp.bfloat16)
        ahead = dot_nn(marks, earlier[...])
        rank = jnp.sum(to_dest * ahead[:8], axis=0, keepdims=True)
        within = [jnp.sum(picks[j] * ahead[8:], axis=0, keepdims=True) for j in range(TOP)]
        return table, dest, at_me, local, rank, within

    def slot_tables(k, ranked):
        table, dest, at_me, local, rank, within = ranked
        row_key = jnp.where(at_me, rank, -1.0)
        picked = one_hot(iota_f32((row_cap, span), 0) == row_key)
        columns = jnp.zeros((8, span), jnp.float32)
        entries = [local[0] + 1.0, within[0], local[1] + 1.0, within[1]]
        entries += [table[3 + i : 4 + i] for i in range(4)]
        for i, entry in enumerate(entries):
            columns = jnp.where(kinds == float(i), entry, columns)
        columns = jnp.concatenate([columns, jnp.zeros((8, span), jnp.float32)], axis=0)
        columns = columns.astype(jnp.bfloat16)
        across_rows = dot_nt(columns, picked)
        along_rows = dot_nt(picked, columns)
        slot_ids = iota_f32((n_slots, row_cap), 0)
        slot_lanes = iota_f32((row_cap, n_slots), 1)
        lane_hits = []
        gains = 0.0
        hot = 0.0
        for j in range(TOP):
            level = across_rows[2 * j : 2 * j + 1]
            slot = jnp.where(
                level > 0.5, (level - 1.0) * capacity + across_rows[2 * j + 1 : 2 * j + 2], -1.0
            )
            weight = across_rows[4 + 2 * j : 5 + 2 * j] + across_rows[5 + 2 * j : 6 + 2 * j]
            match = slot_ids == slot
            hot = hot + jnp.where(match, 1.0, 0.0)
            gains = gains + jnp.where(match, weight, 0.0)
            level = along_rows[:, 2 * j : 2 * j + 1]
            slot = jnp.where(
                level > 0.5, (level - 1.0) * capacity + along_rows[:, 2 * j + 1 : 2 * j + 2], -1.0
            )
            lane_hits.append(jnp.where(slot_lanes == slot, 1.0, 0.0))
        gather_hot[k] = hot.astype(jnp.bfloat16)
        return_hot[k] = (lane_hits[0] + lane_hits[1]).astype(jnp.bfloat16)
        slot_weight[k] = jnp.sum(gains, axis=1, keepdims=True)

    get_x.wait()
    get_xg.wait()
    weights = []
    for e in range(exp_dev):
        for i, (src, dst) in enumerate(((wg_hbm, wg), (wu_hbm, wu), (wd_hbm, wd))):
            copy = pltpu.make_async_copy(src.at[e], dst.at[e], w_sem.at[i, e])
            copy.start()
            weights.append(copy)

    norm_rows = 32

    def norm_tile(i, carry):
        rows = rows_of(i, norm_rows)
        normed[rows, :] = norm_heads(x_in[rows, :].astype(jnp.float32), xg[...])
        return carry

    lax.fori_loop(0, span // norm_rows, norm_tile, 0, unroll=2)
    own = ranks(0)
    _, dest, _, _, rank, _ = own
    token_key = dest * row_cap + rank
    part_base = (mine * part).astype(jnp.float32)
    part_rows = iota_f32((part, span), 0) + part_base
    chosen = []
    for k in order:
        base = ((me + n_ep - k) % n_ep * row_cap).astype(jnp.float32)
        chosen.append(jnp.where(part_rows + base == token_key, 1.0, 0.0))
    chosen = jnp.concatenate(chosen, axis=0).astype(jnp.bfloat16)
    col = 256

    def send_tile(i, carry):
        cols = rows_of(i, col)
        rows = dot_nn(chosen, normed[:, cols]).astype(jnp.bfloat16)
        for p in range(n_ep - 1):
            send_rows[p, :, cols] = rows[p * part : (p + 1) * part]
        return carry

    lax.fori_loop(0, width // col, send_tile, 0, unroll=2)
    along = []
    for p, k in enumerate(order):
        copy = remote(
            send_rows.at[p],
            arrived.at[n_ep - k, mine],
            z_send.at[n_ep - k],
            z_recv.at[n_ep - k],
            {"ep": (me + n_ep - k) % n_ep},
        )
        copy.start()
        along.append(copy)

    own_rows = one_hot(
        iota_f32((row_cap, span), 0) + (me * row_cap).astype(jnp.float32) == token_key
    )

    def own_tile(i, carry):
        cols = rows_of(i, col)
        rows = dot_nn(own_rows, normed[:, cols]).astype(jnp.bfloat16)
        for p in range(n_tp):
            arrived[0, p, :, cols] = rows[p * part : (p + 1) * part]
        return carry

    lax.fori_loop(0, width // col, own_tile, 0, unroll=2)

    get_q.wait()
    get_qg.wait()
    get_lf.wait()
    for h in range(heads):
        q_norm[h] = norm_heads(
            q_in[:, h * head : (h + 1) * head].astype(jnp.float32), qg[...]
        )
    tile = 256
    first_token = pl.multiple_of(me * span, span)

    def attend(d):
        key_start = pl.multiple_of((me - d) * span, span)
        for h in range(heads):
            start_gate = lf[h : h + 1, pl.ds(first_token, head)][:, 0:1]
            gate = (start_gate - lf[h : h + 1, pl.ds(key_start, span)]) * LOG2E

            def query_tile(i, carry):
                rows = rows_of(i, tile)
                scores = dot_nt(q_norm[h, rows, :], kv[d, 0]) * score_scale + gate
                if d == 0:
                    key_at = lax.broadcasted_iota(jnp.int32, (tile, span), 1)
                    query_at = lax.broadcasted_iota(jnp.int32, (tile, span), 0) + i * tile
                    scores = jnp.where(key_at <= query_at, scores, -jnp.inf)
                top = jnp.max(scores, axis=-1, keepdims=True)
                if d == 0:
                    prob = jnp.exp2(scores - top)
                    run_max[h, rows, :] = top
                    run_sum[h, rows, :] = jnp.sum(prob, axis=-1, keepdims=True)
                    run_acc[h, rows, :] = dot_nn(prob.astype(jnp.bfloat16), kv[d, 1])
                else:
                    old = run_max[h, rows, :]
                    top = jnp.maximum(old, top)
                    shrink = jnp.exp2(old - top)
                    prob = jnp.exp2(scores - top)
                    run_max[h, rows, :] = top
                    run_sum[h, rows, :] = run_sum[h, rows, :] * shrink + jnp.sum(
                        prob, axis=-1, keepdims=True
                    )
                    run_acc[h, rows, :] = run_acc[h, rows, :] * shrink + dot_nn(
                        prob.astype(jnp.bfloat16), kv[d, 1]
                    )
                return carry

            lax.fori_loop(0, span // tile, query_tile, 0, unroll=2)

    def kv_forward(d):
        for i in range(2):

            @pl.when(me >= d)
            def _():
                kv_copies[d - 1][i].wait_recv()

            if d < n_ep - 1:
                kv_pass(d, i)

    def kv_attend(d):
        @pl.when(me >= d)
        def _():
            attend(d)

    inner = (me > 0) & (me < n_ep - 1)
    arrivals = []
    crossing = []
    pairing = []
    for k in order:
        place = arrived.at[k, mine]
        relayed = arrived.at[k, across]
        arrivals.append(
            remote(place, place, z_send.at[k], z_recv.at[k], {"ep": (me + k) % n_ep})
        )
        crossing.append(remote(place, place, x_send.at[k], x_recv.at[k], {"tp": across}))
        pairing.append(
            [
                remote(block, block, c_send.at[i, k], c_recv.at[i, k], {"tp": pair})
                for i, block in enumerate((place, relayed))
            ]
        )

    def only(condition, *steps):
        @pl.when(condition)
        def _():
            for step in steps:
                step[0](*step[1:])

    def pass_on(p):
        arrivals[p].wait_recv()
        crossing[p].start()
        pairing[p][0].start()

    def relay(p):
        crossing[p].wait_recv()
        pairing[p][1].start()

    def fill_slots(p, side):
        k = 0 if p is None else order[p]
        if p is not None:
            pairing[p][0].wait_recv()
            pairing[p][1].wait_recv()

        def slot_tile(i, carry):
            cols = rows_of(i, col)
            rows = arrived[k, :, :, cols].reshape(row_cap, col)
            filled = dot_nn(gather_hot[k], rows).astype(jnp.bfloat16)
            for e in range(exp_dev):
                slots[e, side * capacity : (side + 1) * capacity, cols] = filled[
                    e * capacity : (e + 1) * capacity
                ]
            return carry

        lax.fori_loop(0, width // col, slot_tile, 0, unroll=2)

    wide = 512

    def expert_pass(sources, first_side, low, high):
        sides = slice(first_side * capacity, (first_side + len(sources)) * capacity)

        def one_expert(e, carry):
            rows = slots[e, sides]
            gate_part = dot_nn(rows, wg[e])
            up_part = dot_nn(rows, wu[e])
            weight = jnp.concatenate(
                [
                    slot_weight[0 if p is None else order[p], rows_of(e, capacity), :]
                    for p in sources
                ], axis=0
            )
            hidden = gate_part / (1.0 + jnp.exp(-gate_part)) * up_part * weight
            hidden = hidden.astype(jnp.bfloat16)
            for c in range(width // wide):
                cols = slice(c * wide, (c + 1) * wide)
                result = dot_nn(hidden, wd[e, :, cols]).astype(jnp.bfloat16)
                for i in range(len(sources)):
                    down[first_side + i, e, :, cols] = result[i * capacity : (i + 1) * capacity]
            return carry

        lax.fori_loop(low, high, one_expert, 0, unroll=2)

    back_pairing = {}
    back_crossing = {}
    back_along = {}

    def combine(p, side):
        k = 0 if p is None else order[p]

        def combine_tile(c, carry):
            cols = rows_of(c, quarter)
            rows = down[side, :, :, cols].reshape(n_slots, quarter)
            partial[k, c] = dot_nn(return_hot[k], rows).astype(jnp.bfloat16)
            return carry

        lax.fori_loop(0, n_tp, combine_tile, 0, unroll=2)
        for way, block in ((1, pair_across), (0, pair)):
            copy = remote(
                partial.at[k, block],
                paired.at[way, k],
                rc_send.at[way, k],
                rc_recv.at[way, k],
                {"tp": pair},
            )
            copy.start()
            back_pairing[way, p] = copy

    rows_half = row_cap // 2

    def back_cross(p, h):
        k = 0 if p is None else order[p]
        if h == 0:
            back_pairing[1, p].wait_recv()
        rows = slice(h * rows_half, (h + 1) * rows_half)
        leaving[k, rows] = (
            partial[k, across, rows].astype(jnp.float32) + paired[1, k, rows].astype(jnp.float32)
        ).astype(jnp.bfloat16)
        back_crossing[p, h].start()

    def back_send(p, h):
        k = 0 if p is None else order[p]
        if h == 0:
            back_pairing[0, p].wait_recv()
        back_crossing[p, h].wait_recv()
        rows = slice(h * rows_half, (h + 1) * rows_half)
        total = partial[k, mine, rows].astype(jnp.float32) + paired[0, k, rows].astype(jnp.float32)
        total = (total + crossed[k, rows].astype(jnp.float32)).astype(jnp.bfloat16)
        if p is None:
            returned[0, rows] = total
            return
        final[k, rows] = total
        back_along[p, h].start()

    for p in (None, 0, 1, 2):
        k = 0 if p is None else order[p]
        for h in range(2):
            rows = pl.ds(h * rows_half, rows_half)
            back_crossing[p, h] = remote(
                leaving.at[k, rows],
                crossed.at[k, rows],
                rx_send.at[k, h],
                rx_recv.at[k, h],
                {"tp": across},
            )
            if p is not None:
                back_along[p, h] = remote(
                    final.at[k, rows],
                    returned.at[k, rows],
                    rz_send.at[k, h],
                    rz_recv.at[k, h],
                    {"ep": (me + n_ep - k) % n_ep},
                )

    mixer_copies = {
        way: remote(mixp.at[block], mpaired.at[way], m_send.at[way], m_recv.at[way], {"tp": pair})
        for way, block in ((1, pair_across), (0, pair))
    }
    half = span // n_tp // 2
    for h in range(2):
        block = slice(h * half, (h + 1) * half)
        mixer_copies[2 + h] = remote(
            mleaving.at[block], mcrossed.at[block], m_send.at[2 + h], m_recv.at[2 + h], {"tp": across}
        )

    def mixer_start():
        for h in range(heads):
            att[:, h * head : (h + 1) * head] = (run_acc[h] / run_sum[h]).astype(jnp.bfloat16)

        def project(c, carry):
            cols = rows_of(c, col)
            rows = dot_nn(att[...], wo[:, cols]).astype(jnp.bfloat16)
            mixp[:, :, cols] = rows.reshape(n_tp, span // n_tp, col)
            return carry

        lax.fori_loop(0, width // col, project, 0, unroll=2)
        mixer_copies[1].start()
        mixer_copies[0].start()

    step = 16

    def mixer_cross(h):
        if h == 0:
            mixer_copies[1].wait_recv()

        def add_tile(i, carry):
            rows = pl.ds(pl.multiple_of(h * half + i * step, step), step)
            mleaving[rows, :] = (
                mixp[across, rows, :].astype(jnp.float32) + mpaired[1, rows, :].astype(jnp.float32)
            ).astype(jnp.bfloat16)
            return carry

        lax.fori_loop(0, half // step, add_tile, 0)
        mixer_copies[2 + h].start()

    def mixer_end():
        mixer_copies[0].wait_recv()
        mixer_copies[2].wait_recv()
        mixer_copies[3].wait_recv()

        def add_tile(i, carry):
            rows = rows_of(i, step)
            total = mixp[mine, rows, :].astype(jnp.float32) + mpaired[0, rows, :].astype(
                jnp.float32
            )
            mix_ref[rows, :] = (total + mcrossed[rows, :].astype(jnp.float32)).astype(
                jnp.bfloat16
            )
            return carry

        lax.fori_loop(0, span // n_tp // step, add_tile, 0)

    outer = jnp.logical_not(inner)
    last = n_ep - 1
    attend(0)
    get_wo.wait()
    only(me == 0, (mixer_start,))
    slot_tables(0, own)
    fill_slots(None, 0)
    pass_on(0)
    for k in range(1, n_ep):
        notes_sent[k - 1].wait_recv()
        slot_tables(k, ranks(k))
    only(inner, (kv_copies[0][1].start,))
    for copy in weights:
        copy.wait()
    split = exp_dev // 2
    expert_pass((None,), 0, 0, split)
    relay(0)
    only(inner, (pass_on, 1))
    only(me == 0, (mixer_cross, 0))
    expert_pass((None,), 0, split, exp_dev)
    combine(None, 0)
    fill_slots(0, 1)
    back_cross(None, 0)
    back_cross(None, 1)
    only(me == 1, (kv_forward, 1))
    only(inner, (pass_on, 2))
    expert_pass((0,), 1, 0, split)
    only(outer, (pass_on, 1))
    only(inner, (relay, 1))
    expert_pass((0,), 1, split, exp_dev)
    combine(0, 1)
    only(outer, (pass_on, 2))
    only(me > 1, (kv_forward, 1))
    only(inner, (back_cross, 0, 0), (back_cross, 0, 1))
    only(me > 0, (attend, 1))
    only(outer, (relay, 1))
    only(inner, (relay, 2))
    fill_slots(1, 0)
    only(me == 0, (mixer_cross, 1))
    only(me == 1, (mixer_start,))
    only(me > 1, (kv_forward, 2), (attend, 2))
    only(outer, (relay, 2), (back_cross, 0, 0), (back_cross, 0, 1))
    only(me == 1, (mixer_cross, 0))
    fill_slots(2, 1)
    expert_pass((1, 2), 0, 0, split)
    only(inner, (back_send, 0, 0), (back_send, 0, 1))
    expert_pass((1, 2), 0, split, exp_dev)
    only(outer, (back_send, 0, 0), (back_send, 0, 1))
    combine(1, 0)
    combine(2, 1)
    back_cross(1, 0)
    back_cross(1, 1)
    only(me == 3, (kv_forward, 3), (attend, 3))
    only(me > 1, (mixer_start,))
    back_send(1, 0)
    back_cross(2, 0)
    back_send(1, 1)
    back_cross(2, 1)
    back_send(None, 0)
    back_send(None, 1)
    only(me > 1, (mixer_cross, 0))
    back_send(2, 0)
    back_send(2, 1)
    only(me > 0, (mixer_cross, 1))
    token_column = jnp.transpose(jnp.broadcast_to(token_key, (8, span)), (1, 0))[:, 0:1]
    for k in range(n_ep):
        base = ((me + k) % n_ep * row_cap).astype(jnp.float32)
        final_hot[k] = one_hot(
            iota_f32((span, row_cap), 1) + base == token_column
        )
    for p in (None, 0, 1, 2):
        k = 0 if p is None else order[p]
        if p is not None:
            for h in range(2):
                back_along[p, h].wait_recv()

        def output_tile(i, carry):
            rows = rows_of(i, 128)
            total = dot_nn(final_hot[k, rows, :], returned[k])
            if p is not None:
                total = total + exp_acc[rows, :]
            if p == n_ep - 2:
                exp_ref[rows, :] = total.astype(jnp.bfloat16)
            else:
                exp_acc[rows, :] = total
            return carry

        lax.fori_loop(0, span // 128, output_tile, 0, unroll=2)
    mixer_end()

    for copy in notes_sent:
        copy.wait_send()
    for d in range(n_ep - 1):

        @pl.when((me >= d) & (me < n_ep - 1))
        def _():
            for copy in kv_copies[d]:
                copy.wait_send()

    for copy in along + crossing + pairing[0] + pairing[1] + pairing[2]:
        copy.wait_send()
    for group in (back_pairing, back_crossing, back_along, mixer_copies):
        for copy in group.values():
            copy.wait_send()


def fused_half(
    queries,
    key_rows,
    value_rows,
    query_gain,
    key_gain,
    log_forget,
    out_weight,
    expert_rows,
    expert_gain,
    routes,
    route_weight,
    gate_weight,
    up_weight,
    down_weight,
    capacity,
):
    n_tp = lax.axis_size("tp")
    n_ep = lax.axis_size("ep")
    span, width = expert_rows.shape
    exp_dev = gate_weight.shape[0]
    hidden = gate_weight.shape[2]
    heads = queries.shape[1] // HEAD_SIZE
    row_cap = exp_dev * capacity // TOP
    part = row_cap // n_tp
    quarter = width // n_tp
    n_slots = exp_dev * capacity
    whole = log_forget.shape[1]
    low = jnp.bfloat16
    full = jnp.float32
    vmem = pltpu.VMEM
    dma = pltpu.SemaphoreType.DMA
    scratch = [
        vmem((span, heads * HEAD_SIZE), low),
        vmem((span, HEAD_SIZE), low),
        vmem((n_ep, 2, span, HEAD_SIZE), low),
        vmem((1, HEAD_SIZE), full),
        vmem((1, HEAD_SIZE), full),
        vmem((heads, whole), full),
        vmem((heads * HEAD_SIZE, width), low),
        vmem((span, width), low),
        vmem((1, width), full),
        vmem((TOP, span), jnp.int32),
        vmem((TOP, span), full),
        vmem((n_ep, 8, span), full),
        vmem((exp_dev, width, hidden), low),
        vmem((exp_dev, width, hidden), low),
        vmem((exp_dev, hidden, width), low),
        vmem((heads, span, HEAD_SIZE), low),
        vmem((heads, span, 1), full),
        vmem((heads, span, 1), full),
        vmem((heads, span, HEAD_SIZE), full),
        vmem((span, heads * HEAD_SIZE), low),
        vmem((n_tp, span // n_tp, width), low),
        vmem((2, span // n_tp, width), low),
        vmem((span // n_tp, width), low),
        vmem((span // n_tp, width), low),
        vmem((span, width), low),
        vmem((span, span), low),
        vmem((n_ep - 1, part, width), low),
        vmem((n_ep, n_tp, part, width), low),
        vmem((n_ep, n_slots, row_cap), low),
        vmem((n_ep, row_cap, n_slots), low),
        vmem((n_ep, n_slots, 1), full),
        vmem((n_ep, span, row_cap), low),
        vmem((span, quarter), full),
        vmem((exp_dev, 2 * capacity, width), low),
        vmem((2, exp_dev, capacity, width), low),
        vmem((n_ep, n_tp, row_cap, quarter), low),
        vmem((2, n_ep, row_cap, quarter), low),
        vmem((n_ep, row_cap, quarter), low),
        vmem((n_ep, row_cap, quarter), low),
        vmem((n_ep, row_cap, quarter), low),
        vmem((n_ep, row_cap, quarter), low),
        dma((11,)),
        dma((3, exp_dev)),
        dma((n_ep, 2)),
        dma((n_ep, 2)),
        dma((n_ep,)),
        dma((n_ep,)),
        dma((n_ep,)),
        dma((n_ep,)),
        dma((n_ep,)),
        dma((n_ep,)),
        dma((2, n_ep)),
        dma((2, n_ep)),
        dma((2, n_ep)),
        dma((2, n_ep)),
        dma((n_ep, 2)),
        dma((n_ep, 2)),
        dma((n_ep, 2)),
        dma((n_ep, 2)),
        dma((4,)),
        dma((4,)),
    ]
    mixed, combined = pl.pallas_call(
        functools.partial(fused_kernel, n_ep, n_tp, capacity),
        out_shape=(
            jax.ShapeDtypeStruct((span // n_tp, width), low),
            jax.ShapeDtypeStruct((span, quarter), low),
        ),
        in_specs=[pl.BlockSpec(memory_space=pl.ANY)] * 14,
        out_specs=(
            pl.BlockSpec(memory_space=pltpu.VMEM),
            pl.BlockSpec(memory_space=pltpu.VMEM),
        ),
        scratch_shapes=scratch,
        compiler_params=pltpu.CompilerParams(
            collective_id=0, has_side_effects=True, vmem_limit_bytes=VMEM_LIMIT
        ),
    )(
        queries,
        key_rows,
        value_rows,
        query_gain.reshape(1, -1),
        key_gain.reshape(1, -1),
        log_forget,
        out_weight,
        expert_rows,
        expert_gain.reshape(1, -1),
        routes,
        route_weight,
        gate_weight,
        up_weight,
        down_weight,
    )
    return settle(mixed, combined)


def settle_kernel(first_in, second_in, first_out, second_out, first, second, sems):
    loads = []
    for i, (src, dst) in enumerate(((first_in, first), (second_in, second))):
        rows = dst.shape[0] // PIECES
        for c in range(PIECES):
            piece = pl.ds(c * rows, rows)
            copy = pltpu.make_async_copy(src.at[piece], dst.at[piece], sems.at[0, i, c])
            copy.start()
            loads.append((i, c, piece, copy))
    stores = []
    for i, c, piece, load in loads:
        load.wait()
        src, dst = ((first, first_out), (second, second_out))[i]
        copy = pltpu.make_async_copy(src.at[piece], dst.at[piece], sems.at[1, i, c])
        copy.start()
        stores.append(copy)
    for copy in stores:
        copy.wait()


def settle(first, second):
    anywhere = pl.BlockSpec(memory_space=pltpu.HBM)
    return pl.pallas_call(
        settle_kernel,
        out_shape=tuple(jax.ShapeDtypeStruct(a.shape, a.dtype) for a in (first, second)),
        in_specs=[anywhere, anywhere],
        out_specs=(anywhere, anywhere),
        scratch_shapes=[
            pltpu.VMEM(first.shape, first.dtype),
            pltpu.VMEM(second.shape, second.dtype),
            pltpu.SemaphoreType.DMA((2, 2, PIECES)),
        ],
        compiler_params=pltpu.CompilerParams(vmem_limit_bytes=VMEM_LIMIT),
    )(first, second)


def on_device(
    queries,
    key_rows,
    value_rows,
    query_gain,
    key_gain,
    log_forget,
    out_weight,
    expert_rows,
    expert_gain,
    routes,
    route_weight,
    gate_weight,
    up_weight,
    down_weight,
):
    mixer_args = (
        queries,
        key_rows,
        value_rows,
        query_gain,
        key_gain,
        log_forget,
        out_weight,
    )
    expert_args = (
        expert_rows,
        expert_gain,
        routes,
        route_weight,
        gate_weight,
        up_weight,
        down_weight,
    )
    n_tp = lax.axis_size("tp")
    n_ep = lax.axis_size("ep")
    span = expert_rows.shape[0]
    capacity = n_tp * ((3 * (span // n_tp) * TOP + 2 * EXPERTS - 1) // (2 * EXPERTS))
    fits = (
        n_tp == 4
        and n_ep == 4
        and gate_weight.shape[0] == GROUP_SIZE
        and capacity % 16 == 0
        and key_rows.shape[1] == HEAD_SIZE
    )
    if fits:
        return fused_half(*mixer_args, *expert_args, capacity)
    expert_out = experts_half(*expert_args)
    mixer_part = mixer_half(*mixer_args)
    mixer_out = lax.psum_scatter(mixer_part, "tp", scatter_dimension=0, tiled=True)
    return (mixer_out, expert_out)


def solution(mesh):
    in_specs = (
        P(("grp", "ep"), "tp"),
        P(("grp", "ep"), "tp"),
        P(("grp", "ep"), "tp"),
        P(),
        P(),
        P("tp", "grp"),
        P("tp", None),
        P(("grp", "ep"), None),
        P(),
        P(None, ("grp", "ep")),
        P(None, ("grp", "ep")),
        P("ep", None, "tp"),
        P("ep", None, "tp"),
        P("ep", "tp", None),
    )
    out_specs = (P(("grp", "ep", "tp"), None), P(("grp", "ep"), "tp"))
    return jax.shard_map(
        on_device, mesh=mesh, in_specs=in_specs, out_specs=out_specs, check_vma=False
    )
```

```python
import functools

import jax
import jax.numpy as jnp
from jax import lax
from jax.experimental import pallas as pl
from jax.experimental.pallas import tpu as pltpu
from jax.sharding import PartitionSpec as P

HEAD_SIZE = 128
EXPERTS = 32
TOP = 2
GROUP_SIZE = 8
VMEM_LIMIT = 65000 * 1024
PIECES = 2


def head_norm(inputs, scale_gain):
    widened = inputs.astype(jnp.float32)
    factor = lax.rsqrt(jnp.mean(widened * widened, axis=-1, keepdims=True) + 1e-06)
    return widened * factor * scale_gain


def slot_table(chosen, experts_all, capacity):
    n_rows = chosen.shape[0]
    per_row = chosen.shape[1]
    flat_ids = chosen.reshape(-1)
    one_hot = (flat_ids[:, None] == jnp.arange(experts_all, dtype=jnp.int32)[None, :]).astype(
        jnp.int32
    )
    within = jnp.sum((jnp.cumsum(one_hot, axis=0) - 1) * one_hot, axis=1)
    slot_index = flat_ids * capacity + within
    row_of = jnp.arange(n_rows * per_row, dtype=jnp.int32) // per_row
    slot_owner = jnp.full((experts_all * capacity,), n_rows, jnp.int32).at[slot_index].set(row_of)
    return (slot_index.reshape(n_rows, per_row), slot_owner)


def mixer_half(queries, key_rows, value_rows, query_gain, key_gain, log_forget, out_weight):
    span_rows = queries.shape[0]
    heads_dev = queries.shape[1] // HEAD_SIZE
    kv_dev = key_rows.shape[1] // HEAD_SIZE
    group_ratio = heads_dev // kv_dev
    scale_qk = HEAD_SIZE ** (-0.5)
    q_normed = head_norm(
        queries.reshape(span_rows, kv_dev, group_ratio, HEAD_SIZE), query_gain
    ).astype(jnp.bfloat16)
    k_normed = head_norm(key_rows.reshape(span_rows, kv_dev, HEAD_SIZE), key_gain).astype(
        jnp.bfloat16
    )
    key_value = jnp.concatenate(
        [k_normed.reshape(span_rows, kv_dev * HEAD_SIZE), value_rows], axis=1
    )
    first_row = lax.axis_index("ep") * span_rows
    last_row = first_row + span_rows - 1
    query_pos = first_row + jnp.arange(span_rows, dtype=jnp.int32)
    query_gates = lax.dynamic_slice_in_dim(log_forget, first_row, span_rows, 1)
    query_gates = query_gates.T.reshape(span_rows, kv_dev, group_ratio)

    def add_block(running, kv_block, key_start):
        run_max, run_sum, run_acc = running
        block_len = kv_block.shape[0]
        k_block = kv_block[:, : kv_dev * HEAD_SIZE].reshape(block_len, kv_dev, HEAD_SIZE)
        v_block = kv_block[:, kv_dev * HEAD_SIZE :].reshape(block_len, kv_dev, HEAD_SIZE)
        key_gates = lax.dynamic_slice_in_dim(log_forget, key_start, block_len, 1)
        key_gates = key_gates.reshape(kv_dev, group_ratio, block_len)
        scores = (
            jnp.einsum("qgrd,kgd->qgrk", q_normed, k_block, preferred_element_type=jnp.float32)
            * scale_qk
        )
        scores = scores + query_gates[..., None] - key_gates[None]
        key_pos = key_start + jnp.arange(block_len, dtype=jnp.int32)
        visible = key_pos[None, :] <= query_pos[:, None]
        scores = jnp.where(visible[:, None, None, :], scores, -jnp.inf)
        new_max = jnp.maximum(run_max, jnp.max(scores, axis=-1))
        shrink = jnp.exp(run_max - new_max)
        weights = jnp.exp(scores - new_max[..., None])
        run_sum = shrink * run_sum + jnp.sum(weights, axis=-1)
        gathered = jnp.einsum(
            "qgrk,kgd->qgrd",
            weights.astype(jnp.bfloat16),
            v_block,
            preferred_element_type=jnp.float32,
        )
        return (new_max, run_sum, shrink[..., None] * run_acc + gathered)

    start_state = (
        jnp.full((span_rows, kv_dev, group_ratio), -jnp.inf, jnp.float32),
        jnp.zeros((span_rows, kv_dev, group_ratio), jnp.float32),
        jnp.zeros((span_rows, kv_dev, group_ratio, HEAD_SIZE), jnp.float32),
    )
    kv_piece = lax.all_gather(key_value, "ep", axis=0, tiled=True)
    block_len = min(kv_piece.shape[0], span_rows)
    n_blocks = kv_piece.shape[0] // block_len

    def one_block(block_number, running_in):
        key_start = block_number * block_len
        kv_block = lax.dynamic_slice_in_dim(kv_piece, block_number * block_len, block_len, 0)

        def take_block(running_now):
            return add_block(running_now, kv_block, key_start)

        def skip_block(running_now):
            return running_now

        return lax.cond(key_start <= last_row, take_block, skip_block, running_in)

    run_max, run_sum, run_acc = lax.fori_loop(0, n_blocks, one_block, start_state)
    attended = (
        (run_acc / run_sum[..., None])
        .astype(jnp.bfloat16)
        .reshape(span_rows, heads_dev * HEAD_SIZE)
    )
    return jnp.dot(attended, out_weight, preferred_element_type=jnp.float32).astype(jnp.bfloat16)


def experts_half(
    expert_rows, expert_gain, routes, route_weight, gate_weight, up_weight, down_weight
):
    n_tp = lax.axis_size("tp")
    n_ep = lax.axis_size("ep")
    span_rows = expert_rows.shape[0]
    model_width = expert_rows.shape[1]
    exp_dev = gate_weight.shape[0]
    capacity = n_tp * ((3 * (span_rows // n_tp) * TOP + 2 * EXPERTS - 1) // (2 * EXPERTS))
    normed = head_norm(expert_rows, expert_gain).astype(jnp.bfloat16)
    slot_index, slot_owner = slot_table(routes.T, EXPERTS, capacity)
    padded = jnp.concatenate([normed, jnp.zeros((1, model_width), jnp.bfloat16)], axis=0)
    part_len = capacity // n_tp
    owner_part = lax.dynamic_slice_in_dim(
        slot_owner.reshape(EXPERTS, capacity), lax.axis_index("tp") * part_len, part_len, 1
    )
    send_rows = padded[owner_part].reshape(n_ep, exp_dev, part_len, model_width)
    arrived = lax.all_to_all(send_rows, "ep", split_axis=0, concat_axis=0, tiled=True)
    slot_rows = lax.all_gather(arrived, "tp", axis=2, tiled=True)
    gate_part = jnp.einsum(
        "nxcd,xdf->nxcf", slot_rows, gate_weight, preferred_element_type=jnp.float32
    )
    up_part = jnp.einsum("nxcd,xdf->nxcf", slot_rows, up_weight, preferred_element_type=jnp.float32)
    hidden = (jax.nn.silu(gate_part) * up_part).astype(jnp.bfloat16)
    partial_out = jnp.einsum(
        "nxcf,xfd->nxcd", hidden, down_weight, preferred_element_type=jnp.float32
    )
    summed = lax.psum_scatter(
        partial_out.astype(jnp.bfloat16), "tp", scatter_dimension=3, tiled=True
    )
    returned = lax.all_to_all(summed, "ep", split_axis=0, concat_axis=0, tiled=True)
    result_table = returned.reshape(EXPERTS * capacity, returned.shape[3])
    picked = result_table[slot_index]
    combined = jnp.sum(picked.astype(jnp.float32) * route_weight.T[..., None], axis=1)
    return combined.astype(jnp.bfloat16)


LOG2E = 1.4426950408889634


def remote(src, dst, send_sem, recv_sem, peer):
    return pltpu.make_async_remote_copy(
        src_ref=src,
        dst_ref=dst,
        send_sem=send_sem,
        recv_sem=recv_sem,
        device_id=peer,
        device_id_type=pl.DeviceIdType.MESH,
    )


def dot_nt(lhs, rhs):
    return lax.dot_general(
        lhs, rhs, (((1,), (1,)), ((), ())), preferred_element_type=jnp.float32
    )


def dot_nn(lhs, rhs):
    return jnp.dot(lhs, rhs, preferred_element_type=jnp.float32)


def rows_of(index, size):
    return pl.ds(pl.multiple_of(index * size, size), size)


def one_hot(condition):
    return jnp.where(condition, 1.0, 0.0).astype(jnp.bfloat16)


def iota_f32(shape, dim):
    return lax.broadcasted_iota(jnp.int32, shape, dim).astype(jnp.float32)


def fused_kernel(
    n_ep,
    n_tp,
    capacity,
    q_hbm,
    k_hbm,
    v_hbm,
    qg_hbm,
    kg_hbm,
    lf_hbm,
    wo_hbm,
    x_hbm,
    xg_hbm,
    routes_hbm,
    share_hbm,
    wg_hbm,
    wu_hbm,
    wd_hbm,
    mix_hbm,
    exp_hbm,
    mix_ref,
    exp_ref,
    q_in,
    k_in,
    kv,
    qg,
    kg,
    lf,
    wo,
    mixp,
    xg,
    routes,
    share,
    info,
    wg,
    wu,
    wd,
    q_norm,
    run_max,
    run_sum,
    run_acc,
    att,
    mpaired,
    mcrossed,
    normed,
    earlier,
    send_rows,
    arrived,
    gather_hot,
    return_hot,
    slot_weight,
    final_hot,
    exp_acc,
    slots,
    down,
    partial,
    paired,
    crossed,
    returned,
    in_sem,
    w_sem,
    kv_send,
    kv_recv,
    i_send,
    i_recv,
    z_send,
    z_recv,
    x_send,
    x_recv,
    c_send,
    c_recv,
    rc_send,
    rc_recv,
    rx_send,
    rx_recv,
    rz_send,
    rz_recv,
    m_send,
    m_recv,
    out_sem,
):
    me = lax.axis_index("ep")
    mine = lax.axis_index("tp")
    pair = mine + 1 - 2 * (mine % 2)
    across = (mine + n_tp // 2) % n_tp
    pair_across = (pair + n_tp // 2) % n_tp
    span, width = x_hbm.shape
    block_rows = span // n_tp
    heads = q_norm.shape[0]
    head = q_norm.shape[2]
    exp_dev = wg.shape[0]
    part = send_rows.shape[1]
    row_cap = part * n_tp
    lead = (part + 31) // 32 * 16
    chunks = (pl.ds(0, lead), pl.ds(lead, part - lead))
    n_slots = exp_dev * capacity
    quarter = width // n_tp
    score_scale = (head**-0.5) * LOG2E
    near = n_ep - 1 - (n_ep - 2) * (me // (n_ep - 1))
    middle = 2 - me * (n_ep - 1 - me) // 2
    order = (near, middle, 2 * n_ep - 2 - near - middle)

    fetches = []

    def fetch(src, dst):
        copy = pltpu.make_async_copy(src, dst, in_sem.at[len(fetches)])
        copy.start()
        fetches.append(copy)
        return copy

    get_k = fetch(k_hbm, k_in)
    get_kg = fetch(kg_hbm, kg)
    get_v = fetch(v_hbm, kv.at[0, 1])
    get_routes = fetch(routes_hbm, routes)
    get_share = fetch(share_hbm, share)
    get_x = [fetch(x_hbm.at[pl.ds(i * block_rows, block_rows)], mixp.at[i]) for i in range(n_tp)]
    get_xg = fetch(xg_hbm, xg)
    get_q = fetch(q_hbm, q_in)
    get_qg = fetch(qg_hbm, qg)
    get_lf = fetch(lf_hbm, lf)
    get_wo = fetch(wo_hbm, wo)
    barrier = pltpu.get_barrier_semaphore()
    peers = [{"ep": (me + k) % n_ep} for k in range(1, n_ep)] + [{"tp": pair}, {"tp": across}]
    for peer in peers:
        pl.semaphore_signal(barrier, inc=1, device_id=peer, device_id_type=pl.DeviceIdType.MESH)

    get_k.wait()
    get_kg.wait()

    def norm_heads(rows, gain):
        factor = lax.rsqrt(jnp.mean(rows * rows, axis=-1, keepdims=True) + 1e-06)
        return (rows * factor * gain).astype(jnp.bfloat16)

    kv[0, 0] = norm_heads(k_in[...].astype(jnp.float32), kg[...])
    get_routes.wait()
    get_share.wait()
    get_v.wait()
    chosen_ids = routes[...].astype(jnp.float32)
    shares = share[...]
    high = shares.astype(jnp.bfloat16).astype(jnp.float32)
    group = jnp.zeros((1, span), jnp.float32)
    for d in range(1, n_ep):
        group = group + jnp.where(chosen_ids[0:1] >= float(d * exp_dev), 1.0, 0.0)
    kinds = iota_f32((8, span), 0)
    entries = [group] + [chosen_ids[j : j + 1] - group * exp_dev for j in range(TOP)]
    for j in range(TOP):
        entries += [high[j : j + 1], shares[j : j + 1] - high[j : j + 1]]
    table = jnp.zeros((8, span), jnp.float32)
    for i, entry in enumerate(entries):
        table = jnp.where(kinds == float(i), entry, table)
    info[0] = table
    pl.semaphore_wait(barrier, len(peers))

    kv_copies = [
        [
            remote(
                kv.at[d, i],
                kv.at[d + 1, i],
                kv_send.at[d, i],
                kv_recv.at[d + 1, i],
                {"ep": (me + 1) % n_ep},
            )
            for i in range(2)
        ]
        for d in range(n_ep - 1)
    ]

    def kv_pass(d, i):
        @pl.when((me >= d) & (me < n_ep - 1))
        def _():
            kv_copies[d][i].start()

    kv_pass(0, 0)

    @pl.when(me == 0)
    def _():
        kv_copies[0][1].start()

    notes_sent = []
    for k in range(1, n_ep):
        copy = remote(
            info.at[0], info.at[k], i_send.at[k], i_recv.at[k], {"ep": (me + k) % n_ep}
        )
        copy.start()
        notes_sent.append(copy)

    me_f = me.astype(jnp.float32)
    earlier[...] = one_hot(iota_f32((span, span), 0) < iota_f32((span, span), 1))

    def ranks(k):
        table = info[k]
        dest = table[0:1]
        at_me = dest == me_f
        local = [jnp.where(at_me, table[1 + j : 2 + j], -1.0) for j in range(TOP)]
        to_dest = jnp.where(dest == kinds, 1.0, 0.0)
        picks = [jnp.where(local[j] == kinds, 1.0, 0.0) for j in range(TOP)]
        marks = jnp.concatenate([to_dest, picks[0] + picks[1]], axis=0).astype(jnp.bfloat16)
        ahead = dot_nn(marks, earlier[...])
        rank = jnp.sum(to_dest * ahead[:8], axis=0, keepdims=True)
        within = [jnp.sum(picks[j] * ahead[8:], axis=0, keepdims=True) for j in range(TOP)]
        return table, dest, at_me, local, rank, within

    def slot_tables(k, ranked):
        table, dest, at_me, local, rank, within = ranked
        row_key = jnp.where(at_me, rank, -1.0)
        picked = one_hot(iota_f32((row_cap, span), 0) == row_key)
        columns = jnp.zeros((8, span), jnp.float32)
        entries = [local[0] + 1.0, within[0], local[1] + 1.0, within[1]]
        entries += [table[3 + i : 4 + i] for i in range(4)]
        for i, entry in enumerate(entries):
            columns = jnp.where(kinds == float(i), entry, columns)
        columns = jnp.concatenate([columns, jnp.zeros((8, span), jnp.float32)], axis=0)
        columns = columns.astype(jnp.bfloat16)
        across_rows = dot_nt(columns, picked)
        along_rows = dot_nt(picked, columns)
        slot_ids = iota_f32((n_slots, row_cap), 0)
        slot_lanes = iota_f32((row_cap, n_slots), 1)
        lane_hits = []
        gains = 0.0
        hot = 0.0
        for j in range(TOP):
            level = across_rows[2 * j : 2 * j + 1]
            slot = jnp.where(
                level > 0.5, (level - 1.0) * capacity + across_rows[2 * j + 1 : 2 * j + 2], -1.0
            )
            weight = across_rows[4 + 2 * j : 5 + 2 * j] + across_rows[5 + 2 * j : 6 + 2 * j]
            match = slot_ids == slot
            hot = hot + jnp.where(match, 1.0, 0.0)
            gains = gains + jnp.where(match, weight, 0.0)
            level = along_rows[:, 2 * j : 2 * j + 1]
            slot = jnp.where(
                level > 0.5, (level - 1.0) * capacity + along_rows[:, 2 * j + 1 : 2 * j + 2], -1.0
            )
            lane_hits.append(jnp.where(slot_lanes == slot, 1.0, 0.0))
        gather_hot[k] = hot.astype(jnp.bfloat16)
        return_hot[k] = (lane_hits[0] + lane_hits[1]).astype(jnp.bfloat16)
        slot_weight[k] = jnp.sum(gains, axis=1, keepdims=True)

    for copy in get_x:
        copy.wait()
    get_xg.wait()
    weights = []
    for e in range(exp_dev):
        for i, (src, dst) in enumerate(((wg_hbm, wg), (wu_hbm, wu), (wd_hbm, wd))):
            copy = pltpu.make_async_copy(src.at[e], dst.at[e], w_sem.at[i, e])
            copy.start()
            weights.append(copy)

    norm_rows = 32

    def norm_tile(i, carry):
        rows = rows_of(i, norm_rows)
        per = block_rows // norm_rows
        source = mixp[i // per, rows_of(i % per, norm_rows), :]
        normed[rows, :] = norm_heads(source.astype(jnp.float32), xg[...])
        return carry

    lax.fori_loop(0, span // norm_rows, norm_tile, 0, unroll=2)
    own = ranks(0)
    _, dest, _, _, rank, _ = own
    token_key = dest * row_cap + rank
    part_base = (mine * part).astype(jnp.float32)
    part_rows = iota_f32((part, span), 0) + part_base
    chosen = []
    for k in order:
        base = ((me + n_ep - k) % n_ep * row_cap).astype(jnp.float32)
        chosen.append(jnp.where(part_rows + base == token_key, 1.0, 0.0))
    chosen = jnp.concatenate(chosen, axis=0).astype(jnp.bfloat16)
    col = 256

    def send_tile(i, carry):
        cols = rows_of(i, col)
        rows = dot_nn(chosen, normed[:, cols]).astype(jnp.bfloat16)
        for p in range(n_ep - 1):
            send_rows[p, :, cols] = rows[p * part : (p + 1) * part]
        return carry

    lax.fori_loop(0, width // col, send_tile, 0, unroll=2)
    along = []
    for p, k in enumerate(order):
        for h, rows in enumerate(chunks):
            copy = remote(
                send_rows.at[p, rows],
                arrived.at[n_ep - k, mine, rows],
                z_send.at[n_ep - k, h],
                z_recv.at[n_ep - k, h],
                {"ep": (me + n_ep - k) % n_ep},
            )
            copy.start()
            along.append(copy)

    own_rows = one_hot(
        iota_f32((row_cap, span), 0) + (me * row_cap).astype(jnp.float32) == token_key
    )

    def own_tile(i, carry):
        cols = rows_of(i, col)
        rows = dot_nn(own_rows, normed[:, cols]).astype(jnp.bfloat16)
        for p in range(n_tp):
            arrived[0, p, :, cols] = rows[p * part : (p + 1) * part]
        return carry

    lax.fori_loop(0, width // col, own_tile, 0, unroll=2)

    get_q.wait()
    get_qg.wait()
    get_lf.wait()
    for h in range(heads):
        q_norm[h] = norm_heads(
            q_in[:, h * head : (h + 1) * head].astype(jnp.float32), qg[...]
        )
    tile = 256
    first_token = pl.multiple_of(me * span, span)

    def attend(d):
        key_start = pl.multiple_of((me - d) * span, span)
        for h in range(heads):
            start_gate = lf[h : h + 1, pl.ds(first_token, head)][:, 0:1]
            gate = (start_gate - lf[h : h + 1, pl.ds(key_start, span)]) * LOG2E

            def query_tile(i, carry):
                rows = rows_of(i, tile)
                scores = dot_nt(q_norm[h, rows, :], kv[d, 0]) * score_scale + gate
                if d == 0:
                    key_at = lax.broadcasted_iota(jnp.int32, (tile, span), 1)
                    query_at = lax.broadcasted_iota(jnp.int32, (tile, span), 0) + i * tile
                    scores = jnp.where(key_at <= query_at, scores, -jnp.inf)
                top = jnp.max(scores, axis=-1, keepdims=True)
                if d == 0:
                    prob = jnp.exp2(scores - top)
                    run_max[h, rows, :] = top
                    run_sum[h, rows, :] = jnp.sum(prob, axis=-1, keepdims=True)
                    run_acc[h, rows, :] = dot_nn(prob.astype(jnp.bfloat16), kv[d, 1])
                else:
                    old = run_max[h, rows, :]
                    top = jnp.maximum(old, top)
                    shrink = jnp.exp2(old - top)
                    prob = jnp.exp2(scores - top)
                    run_max[h, rows, :] = top
                    run_sum[h, rows, :] = run_sum[h, rows, :] * shrink + jnp.sum(
                        prob, axis=-1, keepdims=True
                    )
                    run_acc[h, rows, :] = run_acc[h, rows, :] * shrink + dot_nn(
                        prob.astype(jnp.bfloat16), kv[d, 1]
                    )
                return carry

            lax.fori_loop(0, span // tile, query_tile, 0, unroll=2)

    def kv_forward(d):
        for i in range(2):

            @pl.when(me >= d)
            def _():
                kv_copies[d - 1][i].wait_recv()

            if d < n_ep - 1:
                kv_pass(d, i)

    def kv_attend(d):
        @pl.when(me >= d)
        def _():
            attend(d)

    inner = (me > 0) & (me < n_ep - 1)
    arrivals = []
    crossing = []
    pairing = []
    for k in order:
        for h, rows in enumerate(chunks):
            place = arrived.at[k, mine, rows]
            relayed = arrived.at[k, across, rows]
            arrivals.append(
                remote(place, place, z_send.at[k, h], z_recv.at[k, h], {"ep": (me + k) % n_ep})
            )
            crossing.append(
                remote(place, place, x_send.at[k, h], x_recv.at[k, h], {"tp": across})
            )
            pairing.append(
                [
                    remote(block, block, c_send.at[i, k, h], c_recv.at[i, k, h], {"tp": pair})
                    for i, block in enumerate((place, relayed))
                ]
            )

    def only(condition, *steps):
        @pl.when(condition)
        def _():
            for step in steps:
                step[0](*step[1:])

    def pass_on(p, h):
        arrivals[2 * p + h].wait_recv()
        crossing[2 * p + h].start()
        pairing[2 * p + h][0].start()

    def relay(p, h):
        crossing[2 * p + h].wait_recv()
        pairing[2 * p + h][1].start()

    def fill_slots(p, side):
        k = 0 if p is None else order[p]
        if p is not None:
            for h in range(2):
                pairing[2 * p + h][0].wait_recv()
                pairing[2 * p + h][1].wait_recv()

        def slot_tile(i, carry):
            cols = rows_of(i, col)
            rows = arrived[k, :, :, cols].reshape(row_cap, col)
            filled = dot_nn(gather_hot[k], rows).astype(jnp.bfloat16)
            for e in range(exp_dev):
                slots[e, side * capacity : (side + 1) * capacity, cols] = filled[
                    e * capacity : (e + 1) * capacity
                ]
            return carry

        lax.fori_loop(0, width // col, slot_tile, 0, unroll=2)

    wide = 512

    def expert_pass(sources, first_side, low, high):
        sides = slice(first_side * capacity, (first_side + len(sources)) * capacity)

        def one_expert(e, carry):
            rows = slots[e, sides]
            gate_part = dot_nn(rows, wg[e])
            up_part = dot_nn(rows, wu[e])
            weight = jnp.concatenate(
                [
                    slot_weight[0 if p is None else order[p], rows_of(e, capacity), :]
                    for p in sources
                ], axis=0
            )
            hidden = gate_part / (1.0 + jnp.exp(-gate_part)) * up_part * weight
            hidden = hidden.astype(jnp.bfloat16)
            for c in range(width // wide):
                cols = slice(c * wide, (c + 1) * wide)
                result = dot_nn(hidden, wd[e, :, cols]).astype(jnp.bfloat16)
                for i in range(len(sources)):
                    down[first_side + i, e, :, cols] = result[i * capacity : (i + 1) * capacity]
            return carry

        lax.fori_loop(low, high, one_expert, 0, unroll=2)

    back_pairing = {}
    back_crossing = {}
    back_along = {}

    def combine(p, side):
        k = 0 if p is None else order[p]

        def block(c):
            cols = rows_of(c, quarter)
            rows = down[side, :, :, cols].reshape(n_slots, quarter)
            partial[k, c] = dot_nn(return_hot[k], rows).astype(jnp.bfloat16)

        block(pair_across)
        block(pair)
        back_pairing[1, p].start()
        back_pairing[0, p].start()
        block(across)
        block(mine)

    rows_half = row_cap // 2

    def back_cross(p, h):
        k = 0 if p is None else order[p]
        if h == 0:
            back_pairing[1, p].wait_recv()
        rows = slice(h * rows_half, (h + 1) * rows_half)
        partial[k, across, rows] = (
            partial[k, across, rows].astype(jnp.float32) + paired[1, k, rows].astype(jnp.float32)
        ).astype(jnp.bfloat16)
        back_crossing[p, h].start()

    def back_send(p, h):
        k = 0 if p is None else order[p]
        if h == 0:
            back_pairing[0, p].wait_recv()
        back_crossing[p, h].wait_recv()
        rows = slice(h * rows_half, (h + 1) * rows_half)
        total = partial[k, mine, rows].astype(jnp.float32) + paired[0, k, rows].astype(jnp.float32)
        total = (total + crossed[k, rows].astype(jnp.float32)).astype(jnp.bfloat16)
        if p is None:
            returned[0, rows] = total
            return
        partial[k, mine, rows] = total
        back_along[p, h].start()

    for p in (None, 0, 1, 2):
        k = 0 if p is None else order[p]
        for way, side in ((1, pair_across), (0, pair)):
            back_pairing[way, p] = remote(
                partial.at[k, side],
                paired.at[way, k],
                rc_send.at[way, k],
                rc_recv.at[way, k],
                {"tp": pair},
            )
        for h in range(2):
            rows = pl.ds(h * rows_half, rows_half)
            back_crossing[p, h] = remote(
                partial.at[k, across, rows],
                crossed.at[k, rows],
                rx_send.at[k, h],
                rx_recv.at[k, h],
                {"tp": across},
            )
            if p is not None:
                back_along[p, h] = remote(
                    partial.at[k, mine, rows],
                    returned.at[k, rows],
                    rz_send.at[k, h],
                    rz_recv.at[k, h],
                    {"ep": (me + n_ep - k) % n_ep},
                )

    mixer_copies = {
        way: remote(mixp.at[block], mpaired.at[way], m_send.at[way], m_recv.at[way], {"tp": pair})
        for way, block in ((1, pair_across), (0, pair))
    }
    half = span // n_tp // 2
    for h in range(2):
        block = slice(h * half, (h + 1) * half)
        mixer_copies[2 + h] = remote(
            mixp.at[across, block], mcrossed.at[block], m_send.at[2 + h], m_recv.at[2 + h], {"tp": across}
        )

    def mixer_start():
        for h in range(heads):
            att[:, h * head : (h + 1) * head] = (run_acc[h] / run_sum[h]).astype(jnp.bfloat16)

        def project(c, carry):
            cols = rows_of(c, col)
            rows = dot_nn(att[...], wo[:, cols]).astype(jnp.bfloat16)
            mixp[:, :, cols] = rows.reshape(n_tp, span // n_tp, col)
            return carry

        lax.fori_loop(0, width // col, project, 0, unroll=2)
        mixer_copies[1].start()
        mixer_copies[0].start()

    step = 16

    def mixer_cross(h):
        if h == 0:
            mixer_copies[1].wait_recv()

        def add_tile(i, carry):
            rows = pl.ds(pl.multiple_of(h * half + i * step, step), step)
            mixp[across, rows, :] = (
                mixp[across, rows, :].astype(jnp.float32) + mpaired[1, rows, :].astype(jnp.float32)
            ).astype(jnp.bfloat16)
            return carry

        lax.fori_loop(0, half // step, add_tile, 0)
        mixer_copies[2 + h].start()

    outward = []
    for i, (src, dst, size) in enumerate(((mix_ref, mix_hbm, half), (exp_ref, exp_hbm, span // 2))):
        for h in range(2):
            piece = pl.ds(h * size, size)
            outward.append(
                pltpu.make_async_copy(src.at[piece], dst.at[piece], out_sem.at[2 * i + h])
            )

    def mixer_end():
        mixer_copies[0].wait_recv()

        def add_tile(i, carry):
            rows = rows_of(i, step)
            total = mixp[mine, rows, :].astype(jnp.float32) + mpaired[0, rows, :].astype(
                jnp.float32
            )
            mix_ref[rows, :] = (total + mcrossed[rows, :].astype(jnp.float32)).astype(
                jnp.bfloat16
            )
            return carry

        for h in range(2):
            mixer_copies[2 + h].wait_recv()
            lax.fori_loop(h * half // step, (h + 1) * half // step, add_tile, 0, unroll=2)
            outward[h].start()

    outer = jnp.logical_not(inner)
    last = n_ep - 1
    attend(0)
    get_wo.wait()
    only(me == 0, (mixer_start,))
    slot_tables(0, own)
    fill_slots(None, 0)
    split = exp_dev // 2
    for copy in weights[: 3 * split]:
        copy.wait()
    expert_pass((None,), 0, 0, split)
    pass_on(0, 0)
    pass_on(0, 1)
    for copy in weights[3 * split :]:
        copy.wait()
    expert_pass((None,), 0, split, exp_dev)
    combine(None, 0)
    notes_sent[0].wait_recv()
    slot_tables(1, ranks(1))
    only(inner, (pass_on, 1, 0), (pass_on, 1, 1))
    back_cross(None, 0)
    back_cross(None, 1)
    for k in range(2, n_ep):
        notes_sent[k - 1].wait_recv()
        slot_tables(k, ranks(k))
    relay(0, 0)
    relay(0, 1)

    @pl.when(inner)
    def _():
        kv_copies[0][1].start()
        fill_slots(0, 0)
        pass_on(2, 0)
        pass_on(2, 1)
        only(me == 1, (kv_forward, 1), (attend, 1))
        relay(1, 0)
        relay(1, 1)
        only(me == 1, (mixer_start,))
        fill_slots(1, 1)
        expert_pass((0, 1), 0, 0, split)
        only(me == 2, (kv_forward, 1), (attend, 1))
        relay(2, 0)
        relay(2, 1)
        only(me == 1, (mixer_cross, 0))
        expert_pass((0, 1), 0, split, exp_dev)
        combine(0, 0)
        combine(1, 1)
        only(me == 1, (back_cross, 0, 0), (back_cross, 0, 1))
        only(me == 2, (back_cross, 1, 0), (back_cross, 1, 1), (kv_forward, 2))
        fill_slots(2, 0)
        expert_pass((2,), 0, 0, split)
        only(me == 1, (back_cross, 1, 0), (back_cross, 1, 1), (back_send, 0, 0), (back_send, 0, 1))
        only(me == 2, (back_cross, 0, 0), (back_cross, 0, 1), (back_send, 1, 0), (back_send, 1, 1))
        expert_pass((2,), 0, split, exp_dev)
        combine(2, 0)
        only(me == 1, (back_send, 1, 0), (back_send, 1, 1))
        only(me == 2, (back_send, 0, 0), (back_send, 0, 1))
        back_cross(2, 0)
        back_cross(2, 1)
        only(me == 2, (attend, 2), (mixer_start,))
        back_send(None, 0)
        back_send(None, 1)
        only(me == 1, (mixer_cross, 1))
        back_send(2, 0)
        only(me == 2, (mixer_cross, 0))
        back_send(2, 1)
        only(me == 2, (mixer_cross, 1))

    @pl.when(outer)
    def _():
        fill_slots(0, 1)
        step_of = exp_dev // 4
        only(me == 0, (pass_on, 1, 0))
        expert_pass((0,), 1, 0, 2 * step_of)
        only(me == 0, (pass_on, 1, 1))
        only(me == 3, (pass_on, 1, 0))
        expert_pass((0,), 1, 2 * step_of, 3 * step_of)
        only(me == 0, (pass_on, 2, 0))
        only(me == 3, (pass_on, 1, 1))
        expert_pass((0,), 1, 3 * step_of, exp_dev)
        only(me == 3, (pass_on, 2, 0))
        combine(0, 1)
        pass_on(2, 1)
        only(me == 3, (kv_forward, 1), (attend, 1))
        relay(1, 0)
        relay(1, 1)
        fill_slots(1, 0)
        relay(2, 0)
        relay(2, 1)
        back_cross(0, 0)
        back_cross(0, 1)
        only(me == 0, (mixer_cross, 0))
        fill_slots(2, 1)
        expert_pass((1, 2), 0, 0, exp_dev)
        combine(1, 0)
        back_send(0, 0)
        back_send(0, 1)
        combine(2, 1)
        back_cross(1, 0)
        back_cross(1, 1)
        only(me == 3, (kv_forward, 2), (attend, 2), (kv_forward, 3), (attend, 3))
        back_send(1, 0)
        back_cross(2, 0)
        back_send(1, 1)
        back_cross(2, 1)
        back_send(None, 0)
        back_send(None, 1)
        only(me == 0, (mixer_cross, 1))
        only(me == 3, (mixer_start,))
        back_send(2, 0)
        only(me == 3, (mixer_cross, 0))
        back_send(2, 1)
        only(me == 3, (mixer_cross, 1))

    token_column = jnp.transpose(jnp.broadcast_to(token_key, (8, span)), (1, 0))[:, 0:1]
    for k in range(n_ep):
        base = ((me + k) % n_ep * row_cap).astype(jnp.float32)
        final_hot[k] = one_hot(
            iota_f32((span, row_cap), 1) + base == token_column
        )
    for p in (None, 0, 1, 2):
        k = 0 if p is None else order[p]
        if p == 2:
            only(me < 2, (mixer_end,))
        if p is not None:
            for h in range(2):
                back_along[p, h].wait_recv()

        def output_tile(i, carry):
            rows = rows_of(i, 128)
            total = dot_nn(final_hot[k, rows, :], returned[k])
            if p is not None:
                total = total + exp_acc[rows, :]
            if p == 2:
                exp_ref[rows, :] = total.astype(jnp.bfloat16)
            else:
                exp_acc[rows, :] = total
            return carry

        if p == 2:
            for h in range(2):
                lax.fori_loop(h * span // 256, (h + 1) * span // 256, output_tile, 0, unroll=2)
                outward[2 + h].start()
        else:
            lax.fori_loop(0, span // 128, output_tile, 0, unroll=2)
    only(me > 1, (mixer_end,))

    for copy in notes_sent:
        copy.wait_send()
    for copy in outward:
        copy.wait()
    for d in range(n_ep - 1):

        @pl.when((me >= d) & (me < n_ep - 1))
        def _():
            for copy in kv_copies[d]:
                copy.wait_send()

    for copy in along + crossing + sum(pairing, []):
        copy.wait_send()
    for group in (back_pairing, back_crossing, back_along, mixer_copies):
        for copy in group.values():
            copy.wait_send()


def fused_half(
    queries,
    key_rows,
    value_rows,
    query_gain,
    key_gain,
    log_forget,
    out_weight,
    expert_rows,
    expert_gain,
    routes,
    route_weight,
    gate_weight,
    up_weight,
    down_weight,
    capacity,
):
    n_tp = lax.axis_size("tp")
    n_ep = lax.axis_size("ep")
    span, width = expert_rows.shape
    exp_dev = gate_weight.shape[0]
    hidden = gate_weight.shape[2]
    heads = queries.shape[1] // HEAD_SIZE
    row_cap = exp_dev * capacity // TOP
    part = row_cap // n_tp
    quarter = width // n_tp
    n_slots = exp_dev * capacity
    whole = log_forget.shape[1]
    low = jnp.bfloat16
    full = jnp.float32
    vmem = pltpu.VMEM
    dma = pltpu.SemaphoreType.DMA
    scratch = [
        vmem((span // n_tp, width), low),
        vmem((span, quarter), low),
        vmem((span, heads * HEAD_SIZE), low),
        vmem((span, HEAD_SIZE), low),
        vmem((n_ep, 2, span, HEAD_SIZE), low),
        vmem((1, HEAD_SIZE), full),
        vmem((1, HEAD_SIZE), full),
        vmem((heads, whole), full),
        vmem((heads * HEAD_SIZE, width), low),
        vmem((n_tp, span // n_tp, width), low),
        vmem((1, width), full),
        vmem((TOP, span), jnp.int32),
        vmem((TOP, span), full),
        vmem((n_ep, 8, span), full),
        vmem((exp_dev, width, hidden), low),
        vmem((exp_dev, width, hidden), low),
        vmem((exp_dev, hidden, width), low),
        vmem((heads, span, HEAD_SIZE), low),
        vmem((heads, span, 1), full),
        vmem((heads, span, 1), full),
        vmem((heads, span, HEAD_SIZE), full),
        vmem((span, heads * HEAD_SIZE), low),
        vmem((2, span // n_tp, width), low),
        vmem((span // n_tp, width), low),
        vmem((span, width), low),
        vmem((span, span), low),
        vmem((n_ep - 1, part, width), low),
        vmem((n_ep, n_tp, part, width), low),
        vmem((n_ep, n_slots, row_cap), low),
        vmem((n_ep, row_cap, n_slots), low),
        vmem((n_ep, n_slots, 1), full),
        vmem((n_ep, span, row_cap), low),
        vmem((span, quarter), full),
        vmem((exp_dev, 2 * capacity, width), low),
        vmem((2, exp_dev, capacity, width), low),
        vmem((n_ep, n_tp, row_cap, quarter), low),
        vmem((2, n_ep, row_cap, quarter), low),
        vmem((n_ep, row_cap, quarter), low),
        vmem((n_ep, row_cap, quarter), low),
        dma((14,)),
        dma((3, exp_dev)),
        dma((n_ep, 2)),
        dma((n_ep, 2)),
        dma((n_ep,)),
        dma((n_ep,)),
        dma((n_ep, 2)),
        dma((n_ep, 2)),
        dma((n_ep, 2)),
        dma((n_ep, 2)),
        dma((2, n_ep, 2)),
        dma((2, n_ep, 2)),
        dma((2, n_ep)),
        dma((2, n_ep)),
        dma((n_ep, 2)),
        dma((n_ep, 2)),
        dma((n_ep, 2)),
        dma((n_ep, 2)),
        dma((4,)),
        dma((4,)),
        dma((4,)),
    ]
    mixed, combined = pl.pallas_call(
        functools.partial(fused_kernel, n_ep, n_tp, capacity),
        out_shape=(
            jax.ShapeDtypeStruct((span // n_tp, width), low),
            jax.ShapeDtypeStruct((span, quarter), low),
        ),
        in_specs=[pl.BlockSpec(memory_space=pl.ANY)] * 14,
        out_specs=(
            pl.BlockSpec(memory_space=pltpu.HBM),
            pl.BlockSpec(memory_space=pltpu.HBM),
        ),
        scratch_shapes=scratch,
        compiler_params=pltpu.CompilerParams(
            collective_id=0, has_side_effects=True, vmem_limit_bytes=VMEM_LIMIT
        ),
    )(
        queries,
        key_rows,
        value_rows,
        query_gain.reshape(1, -1),
        key_gain.reshape(1, -1),
        log_forget,
        out_weight,
        expert_rows,
        expert_gain.reshape(1, -1),
        routes,
        route_weight,
        gate_weight,
        up_weight,
        down_weight,
    )
    return settle(mixed, combined)


def settle_kernel(first_in, second_in, first_out, second_out, first, second, sems):
    loads = []
    for i, (src, dst) in enumerate(((first_in, first), (second_in, second))):
        rows = dst.shape[0] // PIECES
        for c in range(PIECES):
            piece = pl.ds(c * rows, rows)
            copy = pltpu.make_async_copy(src.at[piece], dst.at[piece], sems.at[0, i, c])
            copy.start()
            loads.append((i, c, piece, copy))
    stores = []
    for i, c, piece, load in loads:
        load.wait()
        src, dst = ((first, first_out), (second, second_out))[i]
        copy = pltpu.make_async_copy(src.at[piece], dst.at[piece], sems.at[1, i, c])
        copy.start()
        stores.append(copy)
    for copy in stores:
        copy.wait()


def settle(first, second):
    anywhere = pl.BlockSpec(memory_space=pltpu.HBM)
    return pl.pallas_call(
        settle_kernel,
        out_shape=tuple(jax.ShapeDtypeStruct(a.shape, a.dtype) for a in (first, second)),
        in_specs=[anywhere, anywhere],
        out_specs=(anywhere, anywhere),
        scratch_shapes=[
            pltpu.VMEM(first.shape, first.dtype),
            pltpu.VMEM(second.shape, second.dtype),
            pltpu.SemaphoreType.DMA((2, 2, PIECES)),
        ],
        compiler_params=pltpu.CompilerParams(vmem_limit_bytes=VMEM_LIMIT),
    )(first, second)


def on_device(
    queries,
    key_rows,
    value_rows,
    query_gain,
    key_gain,
    log_forget,
    out_weight,
    expert_rows,
    expert_gain,
    routes,
    route_weight,
    gate_weight,
    up_weight,
    down_weight,
):
    mixer_args = (
        queries,
        key_rows,
        value_rows,
        query_gain,
        key_gain,
        log_forget,
        out_weight,
    )
    expert_args = (
        expert_rows,
        expert_gain,
        routes,
        route_weight,
        gate_weight,
        up_weight,
        down_weight,
    )
    n_tp = lax.axis_size("tp")
    n_ep = lax.axis_size("ep")
    span = expert_rows.shape[0]
    capacity = n_tp * ((3 * (span // n_tp) * TOP + 2 * EXPERTS - 1) // (2 * EXPERTS))
    fits = (
        n_tp == 4
        and n_ep == 4
        and gate_weight.shape[0] == GROUP_SIZE
        and capacity % 16 == 0
        and key_rows.shape[1] == HEAD_SIZE
    )
    if fits:
        return fused_half(*mixer_args, *expert_args, capacity)
    expert_out = experts_half(*expert_args)
    mixer_part = mixer_half(*mixer_args)
    mixer_out = lax.psum_scatter(mixer_part, "tp", scatter_dimension=0, tiled=True)
    return (mixer_out, expert_out)


def solution(mesh):
    in_specs = (
        P(("grp", "ep"), "tp"),
        P(("grp", "ep"), "tp"),
        P(("grp", "ep"), "tp"),
        P(),
        P(),
        P("tp", "grp"),
        P("tp", None),
        P(("grp", "ep"), None),
        P(),
        P(None, ("grp", "ep")),
        P(None, ("grp", "ep")),
        P("ep", None, "tp"),
        P("ep", None, "tp"),
        P("ep", "tp", None),
    )
    out_specs = (P(("grp", "ep", "tp"), None), P(("grp", "ep"), "tp"))
    return jax.shard_map(
        on_device, mesh=mesh, in_specs=in_specs, out_specs=out_specs, check_vma=False
    )
```

```python
import functools

import jax
import jax.numpy as jnp
from jax import lax
from jax.experimental import pallas as pl
from jax.experimental.pallas import tpu as pltpu
from jax.sharding import PartitionSpec as P

HEAD_SIZE = 128
EXPERTS = 32
TOP = 2
GROUP_SIZE = 8
VMEM_LIMIT = 65000 * 1024
PIECES = 2


def head_norm(inputs, scale_gain):
    widened = inputs.astype(jnp.float32)
    factor = lax.rsqrt(jnp.mean(widened * widened, axis=-1, keepdims=True) + 1e-06)
    return widened * factor * scale_gain


def slot_table(chosen, experts_all, capacity):
    n_rows = chosen.shape[0]
    per_row = chosen.shape[1]
    flat_ids = chosen.reshape(-1)
    one_hot = (flat_ids[:, None] == jnp.arange(experts_all, dtype=jnp.int32)[None, :]).astype(
        jnp.int32
    )
    within = jnp.sum((jnp.cumsum(one_hot, axis=0) - 1) * one_hot, axis=1)
    slot_index = flat_ids * capacity + within
    row_of = jnp.arange(n_rows * per_row, dtype=jnp.int32) // per_row
    slot_owner = jnp.full((experts_all * capacity,), n_rows, jnp.int32).at[slot_index].set(row_of)
    return (slot_index.reshape(n_rows, per_row), slot_owner)


def mixer_half(queries, key_rows, value_rows, query_gain, key_gain, log_forget, out_weight):
    span_rows = queries.shape[0]
    heads_dev = queries.shape[1] // HEAD_SIZE
    kv_dev = key_rows.shape[1] // HEAD_SIZE
    group_ratio = heads_dev // kv_dev
    scale_qk = HEAD_SIZE ** (-0.5)
    q_normed = head_norm(
        queries.reshape(span_rows, kv_dev, group_ratio, HEAD_SIZE), query_gain
    ).astype(jnp.bfloat16)
    k_normed = head_norm(key_rows.reshape(span_rows, kv_dev, HEAD_SIZE), key_gain).astype(
        jnp.bfloat16
    )
    key_value = jnp.concatenate(
        [k_normed.reshape(span_rows, kv_dev * HEAD_SIZE), value_rows], axis=1
    )
    first_row = lax.axis_index("ep") * span_rows
    last_row = first_row + span_rows - 1
    query_pos = first_row + jnp.arange(span_rows, dtype=jnp.int32)
    query_gates = lax.dynamic_slice_in_dim(log_forget, first_row, span_rows, 1)
    query_gates = query_gates.T.reshape(span_rows, kv_dev, group_ratio)

    def add_block(running, kv_block, key_start):
        run_max, run_sum, run_acc = running
        block_len = kv_block.shape[0]
        k_block = kv_block[:, : kv_dev * HEAD_SIZE].reshape(block_len, kv_dev, HEAD_SIZE)
        v_block = kv_block[:, kv_dev * HEAD_SIZE :].reshape(block_len, kv_dev, HEAD_SIZE)
        key_gates = lax.dynamic_slice_in_dim(log_forget, key_start, block_len, 1)
        key_gates = key_gates.reshape(kv_dev, group_ratio, block_len)
        scores = (
            jnp.einsum("qgrd,kgd->qgrk", q_normed, k_block, preferred_element_type=jnp.float32)
            * scale_qk
        )
        scores = scores + query_gates[..., None] - key_gates[None]
        key_pos = key_start + jnp.arange(block_len, dtype=jnp.int32)
        visible = key_pos[None, :] <= query_pos[:, None]
        scores = jnp.where(visible[:, None, None, :], scores, -jnp.inf)
        new_max = jnp.maximum(run_max, jnp.max(scores, axis=-1))
        shrink = jnp.exp(run_max - new_max)
        weights = jnp.exp(scores - new_max[..., None])
        run_sum = shrink * run_sum + jnp.sum(weights, axis=-1)
        gathered = jnp.einsum(
            "qgrk,kgd->qgrd",
            weights.astype(jnp.bfloat16),
            v_block,
            preferred_element_type=jnp.float32,
        )
        return (new_max, run_sum, shrink[..., None] * run_acc + gathered)

    start_state = (
        jnp.full((span_rows, kv_dev, group_ratio), -jnp.inf, jnp.float32),
        jnp.zeros((span_rows, kv_dev, group_ratio), jnp.float32),
        jnp.zeros((span_rows, kv_dev, group_ratio, HEAD_SIZE), jnp.float32),
    )
    kv_piece = lax.all_gather(key_value, "ep", axis=0, tiled=True)
    block_len = min(kv_piece.shape[0], span_rows)
    n_blocks = kv_piece.shape[0] // block_len

    def one_block(block_number, running_in):
        key_start = block_number * block_len
        kv_block = lax.dynamic_slice_in_dim(kv_piece, block_number * block_len, block_len, 0)

        def take_block(running_now):
            return add_block(running_now, kv_block, key_start)

        def skip_block(running_now):
            return running_now

        return lax.cond(key_start <= last_row, take_block, skip_block, running_in)

    run_max, run_sum, run_acc = lax.fori_loop(0, n_blocks, one_block, start_state)
    attended = (
        (run_acc / run_sum[..., None])
        .astype(jnp.bfloat16)
        .reshape(span_rows, heads_dev * HEAD_SIZE)
    )
    return jnp.dot(attended, out_weight, preferred_element_type=jnp.float32).astype(jnp.bfloat16)


def experts_half(
    expert_rows, expert_gain, routes, route_weight, gate_weight, up_weight, down_weight
):
    n_tp = lax.axis_size("tp")
    n_ep = lax.axis_size("ep")
    span_rows = expert_rows.shape[0]
    model_width = expert_rows.shape[1]
    exp_dev = gate_weight.shape[0]
    capacity = n_tp * ((3 * (span_rows // n_tp) * TOP + 2 * EXPERTS - 1) // (2 * EXPERTS))
    normed = head_norm(expert_rows, expert_gain).astype(jnp.bfloat16)
    slot_index, slot_owner = slot_table(routes.T, EXPERTS, capacity)
    padded = jnp.concatenate([normed, jnp.zeros((1, model_width), jnp.bfloat16)], axis=0)
    part_len = capacity // n_tp
    owner_part = lax.dynamic_slice_in_dim(
        slot_owner.reshape(EXPERTS, capacity), lax.axis_index("tp") * part_len, part_len, 1
    )
    send_rows = padded[owner_part].reshape(n_ep, exp_dev, part_len, model_width)
    arrived = lax.all_to_all(send_rows, "ep", split_axis=0, concat_axis=0, tiled=True)
    slot_rows = lax.all_gather(arrived, "tp", axis=2, tiled=True)
    gate_part = jnp.einsum(
        "nxcd,xdf->nxcf", slot_rows, gate_weight, preferred_element_type=jnp.float32
    )
    up_part = jnp.einsum("nxcd,xdf->nxcf", slot_rows, up_weight, preferred_element_type=jnp.float32)
    hidden = (jax.nn.silu(gate_part) * up_part).astype(jnp.bfloat16)
    partial_out = jnp.einsum(
        "nxcf,xfd->nxcd", hidden, down_weight, preferred_element_type=jnp.float32
    )
    summed = lax.psum_scatter(
        partial_out.astype(jnp.bfloat16), "tp", scatter_dimension=3, tiled=True
    )
    returned = lax.all_to_all(summed, "ep", split_axis=0, concat_axis=0, tiled=True)
    result_table = returned.reshape(EXPERTS * capacity, returned.shape[3])
    picked = result_table[slot_index]
    combined = jnp.sum(picked.astype(jnp.float32) * route_weight.T[..., None], axis=1)
    return combined.astype(jnp.bfloat16)


LOG2E = 1.4426950408889634


def remote(src, dst, send_sem, recv_sem, peer):
    return pltpu.make_async_remote_copy(
        src_ref=src,
        dst_ref=dst,
        send_sem=send_sem,
        recv_sem=recv_sem,
        device_id=peer,
        device_id_type=pl.DeviceIdType.MESH,
    )


def dot_nt(lhs, rhs):
    return lax.dot_general(
        lhs, rhs, (((1,), (1,)), ((), ())), preferred_element_type=jnp.float32
    )


def dot_nn(lhs, rhs):
    return jnp.dot(lhs, rhs, preferred_element_type=jnp.float32)


def rows_of(index, size):
    return pl.ds(pl.multiple_of(index * size, size), size)


def one_hot(condition):
    return jnp.where(condition, 1.0, 0.0).astype(jnp.bfloat16)


def iota_f32(shape, dim):
    return lax.broadcasted_iota(jnp.int32, shape, dim).astype(jnp.float32)


def fused_kernel(
    n_ep,
    n_tp,
    capacity,
    q_hbm,
    k_hbm,
    v_hbm,
    qg_hbm,
    kg_hbm,
    lf_hbm,
    wo_hbm,
    x_hbm,
    xg_hbm,
    routes_hbm,
    share_hbm,
    wg_hbm,
    wu_hbm,
    wd_hbm,
    mix_hbm,
    exp_hbm,
    mix_ref,
    exp_ref,
    q_in,
    k_in,
    kv,
    qg,
    kg,
    lf,
    wo,
    mixp,
    xg,
    routes,
    share,
    info,
    wg,
    wu,
    wd,
    q_norm,
    run_max,
    run_sum,
    run_acc,
    att,
    mpaired,
    mcrossed,
    normed,
    earlier,
    send_rows,
    arrived,
    gather_hot,
    return_hot,
    slot_weight,
    final_hot,
    exp_acc,
    slots,
    down,
    partial,
    paired,
    crossed,
    returned,
    in_sem,
    w_sem,
    kv_send,
    kv_recv,
    i_send,
    i_recv,
    z_send,
    z_recv,
    x_send,
    x_recv,
    c_send,
    c_recv,
    rc_send,
    rc_recv,
    rx_send,
    rx_recv,
    rz_send,
    rz_recv,
    m_send,
    m_recv,
    out_sem,
):
    me = lax.axis_index("ep")
    mine = lax.axis_index("tp")
    pair = mine + 1 - 2 * (mine % 2)
    across = (mine + n_tp // 2) % n_tp
    pair_across = (pair + n_tp // 2) % n_tp
    span, width = x_hbm.shape
    block_rows = span // n_tp
    heads = q_norm.shape[0]
    head = q_norm.shape[2]
    exp_dev = wg.shape[0]
    part = send_rows.shape[1]
    row_cap = part * n_tp
    lead = (part + 31) // 32 * 16
    chunks = (pl.ds(0, lead), pl.ds(lead, part - lead))
    n_slots = exp_dev * capacity
    quarter = width // n_tp
    score_scale = (head**-0.5) * LOG2E
    near = n_ep - 1 - (n_ep - 2) * (me // (n_ep - 1))
    middle = 2 - me * (n_ep - 1 - me) // 2
    order = (near, middle, 2 * n_ep - 2 - near - middle)

    fetches = []

    def fetch(src, dst):
        copy = pltpu.make_async_copy(src, dst, in_sem.at[len(fetches)])
        copy.start()
        fetches.append(copy)
        return copy

    get_k = fetch(k_hbm, k_in)
    get_kg = fetch(kg_hbm, kg)
    get_v = fetch(v_hbm, kv.at[0, 1])
    get_routes = fetch(routes_hbm, routes)
    get_share = fetch(share_hbm, share)
    get_x = [fetch(x_hbm.at[pl.ds(i * block_rows, block_rows)], mixp.at[i]) for i in range(n_tp)]
    get_xg = fetch(xg_hbm, xg)
    get_q = fetch(q_hbm, q_in)
    get_qg = fetch(qg_hbm, qg)
    get_lf = fetch(lf_hbm, lf)
    get_wo = fetch(wo_hbm, wo)
    barrier = pltpu.get_barrier_semaphore()
    peers = [{"ep": (me + k) % n_ep} for k in range(1, n_ep)] + [{"tp": pair}, {"tp": across}]
    for peer in peers:
        pl.semaphore_signal(barrier, inc=1, device_id=peer, device_id_type=pl.DeviceIdType.MESH)

    get_k.wait()
    get_kg.wait()

    def norm_heads(rows, gain):
        factor = lax.rsqrt(jnp.mean(rows * rows, axis=-1, keepdims=True) + 1e-06)
        return (rows * factor * gain).astype(jnp.bfloat16)

    kv[0, 0] = norm_heads(k_in[...].astype(jnp.float32), kg[...])
    get_routes.wait()
    get_share.wait()
    get_v.wait()
    chosen_ids = routes[...].astype(jnp.float32)
    shares = share[...]
    high = shares.astype(jnp.bfloat16).astype(jnp.float32)
    group = jnp.zeros((1, span), jnp.float32)
    for d in range(1, n_ep):
        group = group + jnp.where(chosen_ids[0:1] >= float(d * exp_dev), 1.0, 0.0)
    kinds = iota_f32((8, span), 0)
    entries = [group] + [chosen_ids[j : j + 1] - group * exp_dev for j in range(TOP)]
    for j in range(TOP):
        entries += [high[j : j + 1], shares[j : j + 1] - high[j : j + 1]]
    table = jnp.zeros((8, span), jnp.float32)
    for i, entry in enumerate(entries):
        table = jnp.where(kinds == float(i), entry, table)
    info[0] = table
    pl.semaphore_wait(barrier, len(peers))

    kv_copies = [
        [
            remote(
                kv.at[d, i],
                kv.at[d + 1, i],
                kv_send.at[d, i],
                kv_recv.at[d + 1, i],
                {"ep": (me + 1) % n_ep},
            )
            for i in range(2)
        ]
        for d in range(n_ep - 1)
    ]

    def kv_pass(d, i):
        @pl.when((me >= d) & (me < n_ep - 1))
        def _():
            kv_copies[d][i].start()

    kv_pass(0, 0)

    @pl.when(me == 0)
    def _():
        kv_copies[0][1].start()

    notes_sent = []
    for k in range(1, n_ep):
        copy = remote(
            info.at[0], info.at[k], i_send.at[k], i_recv.at[k], {"ep": (me + k) % n_ep}
        )
        copy.start()
        notes_sent.append(copy)

    me_f = me.astype(jnp.float32)
    earlier[...] = one_hot(iota_f32((span, span), 0) < iota_f32((span, span), 1))

    def ranks(k):
        table = info[k]
        dest = table[0:1]
        at_me = dest == me_f
        local = [jnp.where(at_me, table[1 + j : 2 + j], -1.0) for j in range(TOP)]
        to_dest = jnp.where(dest == kinds, 1.0, 0.0)
        picks = [jnp.where(local[j] == kinds, 1.0, 0.0) for j in range(TOP)]
        marks = jnp.concatenate([to_dest, picks[0] + picks[1]], axis=0).astype(jnp.bfloat16)
        ahead = dot_nn(marks, earlier[...])
        rank = jnp.sum(to_dest * ahead[:8], axis=0, keepdims=True)
        within = [jnp.sum(picks[j] * ahead[8:], axis=0, keepdims=True) for j in range(TOP)]
        return table, dest, at_me, local, rank, within

    def slot_tables(k, ranked):
        table, dest, at_me, local, rank, within = ranked
        row_key = jnp.where(at_me, rank, -1.0)
        picked = one_hot(iota_f32((row_cap, span), 0) == row_key)
        columns = jnp.zeros((8, span), jnp.float32)
        entries = [local[0] + 1.0, within[0], local[1] + 1.0, within[1]]
        entries += [table[3 + i : 4 + i] for i in range(4)]
        for i, entry in enumerate(entries):
            columns = jnp.where(kinds == float(i), entry, columns)
        columns = jnp.concatenate([columns, jnp.zeros((8, span), jnp.float32)], axis=0)
        columns = columns.astype(jnp.bfloat16)
        across_rows = dot_nt(columns, picked)
        along_rows = dot_nt(picked, columns)
        slot_ids = iota_f32((n_slots, row_cap), 0)
        slot_lanes = iota_f32((row_cap, n_slots), 1)
        lane_hits = []
        gains = 0.0
        hot = 0.0
        for j in range(TOP):
            level = across_rows[2 * j : 2 * j + 1]
            slot = jnp.where(
                level > 0.5, (level - 1.0) * capacity + across_rows[2 * j + 1 : 2 * j + 2], -1.0
            )
            weight = across_rows[4 + 2 * j : 5 + 2 * j] + across_rows[5 + 2 * j : 6 + 2 * j]
            match = slot_ids == slot
            hot = hot + jnp.where(match, 1.0, 0.0)
            gains = gains + jnp.where(match, weight, 0.0)
            level = along_rows[:, 2 * j : 2 * j + 1]
            slot = jnp.where(
                level > 0.5, (level - 1.0) * capacity + along_rows[:, 2 * j + 1 : 2 * j + 2], -1.0
            )
            lane_hits.append(jnp.where(slot_lanes == slot, 1.0, 0.0))
        gather_hot[k] = hot.astype(jnp.bfloat16)
        return_hot[k] = (lane_hits[0] + lane_hits[1]).astype(jnp.bfloat16)
        slot_weight[k] = jnp.sum(gains, axis=1, keepdims=True)

    for copy in get_x:
        copy.wait()
    get_xg.wait()
    weights = []
    for e in range(exp_dev):
        for i, (src, dst) in enumerate(((wg_hbm, wg), (wu_hbm, wu), (wd_hbm, wd))):
            copy = pltpu.make_async_copy(src.at[e], dst.at[e], w_sem.at[i, e])
            copy.start()
            weights.append(copy)

    norm_rows = 32

    def norm_tile(i, carry):
        rows = rows_of(i, norm_rows)
        per = block_rows // norm_rows
        source = mixp[i // per, rows_of(i % per, norm_rows), :]
        normed[rows, :] = norm_heads(source.astype(jnp.float32), xg[...])
        return carry

    lax.fori_loop(0, span // norm_rows, norm_tile, 0, unroll=2)
    own = ranks(0)
    _, dest, _, _, rank, _ = own
    token_key = dest * row_cap + rank
    part_base = (mine * part).astype(jnp.float32)
    part_rows = iota_f32((part, span), 0) + part_base
    chosen = []
    for k in order:
        base = ((me + n_ep - k) % n_ep * row_cap).astype(jnp.float32)
        chosen.append(jnp.where(part_rows + base == token_key, 1.0, 0.0))
    chosen = jnp.concatenate(chosen, axis=0).astype(jnp.bfloat16)
    col = 256

    def send_tile(i, carry):
        cols = rows_of(i, col)
        rows = dot_nn(chosen, normed[:, cols]).astype(jnp.bfloat16)
        for p in range(n_ep - 1):
            send_rows[p, :, cols] = rows[p * part : (p + 1) * part]
        return carry

    lax.fori_loop(0, width // col, send_tile, 0, unroll=2)
    along = []
    for p, k in enumerate(order):
        for h, rows in enumerate(chunks):
            copy = remote(
                send_rows.at[p, rows],
                arrived.at[n_ep - k, mine, rows],
                z_send.at[n_ep - k, h],
                z_recv.at[n_ep - k, h],
                {"ep": (me + n_ep - k) % n_ep},
            )
            copy.start()
            along.append(copy)

    own_rows = one_hot(
        iota_f32((row_cap, span), 0) + (me * row_cap).astype(jnp.float32) == token_key
    )

    def own_tile(i, carry):
        cols = rows_of(i, col)
        rows = dot_nn(own_rows, normed[:, cols]).astype(jnp.bfloat16)
        for p in range(n_tp):
            arrived[0, p, :, cols] = rows[p * part : (p + 1) * part]
        return carry

    lax.fori_loop(0, width // col, own_tile, 0, unroll=2)

    get_q.wait()
    get_qg.wait()
    get_lf.wait()
    for h in range(heads):
        q_norm[h] = norm_heads(
            q_in[:, h * head : (h + 1) * head].astype(jnp.float32), qg[...]
        )
    tile = 256
    first_token = pl.multiple_of(me * span, span)

    def attend(d):
        key_start = pl.multiple_of((me - d) * span, span)
        for h in range(heads):
            start_gate = lf[h : h + 1, pl.ds(first_token, head)][:, 0:1]
            gate = (start_gate - lf[h : h + 1, pl.ds(key_start, span)]) * LOG2E

            def query_tile(i, carry):
                rows = rows_of(i, tile)
                scores = dot_nt(q_norm[h, rows, :], kv[d, 0]) * score_scale + gate
                if d == 0:
                    key_at = lax.broadcasted_iota(jnp.int32, (tile, span), 1)
                    query_at = lax.broadcasted_iota(jnp.int32, (tile, span), 0) + i * tile
                    scores = jnp.where(key_at <= query_at, scores, -jnp.inf)
                top = jnp.max(scores, axis=-1, keepdims=True)
                if d == 0:
                    prob = jnp.exp2(scores - top)
                    run_max[h, rows, :] = top
                    run_sum[h, rows, :] = jnp.sum(prob, axis=-1, keepdims=True)
                    run_acc[h, rows, :] = dot_nn(prob.astype(jnp.bfloat16), kv[d, 1])
                else:
                    old = run_max[h, rows, :]
                    top = jnp.maximum(old, top)
                    shrink = jnp.exp2(old - top)
                    prob = jnp.exp2(scores - top)
                    run_max[h, rows, :] = top
                    run_sum[h, rows, :] = run_sum[h, rows, :] * shrink + jnp.sum(
                        prob, axis=-1, keepdims=True
                    )
                    run_acc[h, rows, :] = run_acc[h, rows, :] * shrink + dot_nn(
                        prob.astype(jnp.bfloat16), kv[d, 1]
                    )
                return carry

            lax.fori_loop(0, span // tile, query_tile, 0, unroll=2)

    def kv_forward(d):
        for i in range(2):

            @pl.when(me >= d)
            def _():
                kv_copies[d - 1][i].wait_recv()

            if d < n_ep - 1:
                kv_pass(d, i)

    def kv_attend(d):
        @pl.when(me >= d)
        def _():
            attend(d)

    inner = (me > 0) & (me < n_ep - 1)
    arrivals = []
    crossing = []
    pairing = []
    for k in order:
        for h, rows in enumerate(chunks):
            place = arrived.at[k, mine, rows]
            relayed = arrived.at[k, across, rows]
            arrivals.append(
                remote(place, place, z_send.at[k, h], z_recv.at[k, h], {"ep": (me + k) % n_ep})
            )
            crossing.append(
                remote(place, place, x_send.at[k, h], x_recv.at[k, h], {"tp": across})
            )
            pairing.append(
                [
                    remote(block, block, c_send.at[i, k, h], c_recv.at[i, k, h], {"tp": pair})
                    for i, block in enumerate((place, relayed))
                ]
            )

    def only(condition, *steps):
        @pl.when(condition)
        def _():
            for step in steps:
                step[0](*step[1:])

    def pass_on(p, h):
        arrivals[2 * p + h].wait_recv()
        crossing[2 * p + h].start()
        pairing[2 * p + h][0].start()

    def relay(p, h):
        crossing[2 * p + h].wait_recv()
        pairing[2 * p + h][1].start()

    def fill_slots(p, side):
        k = 0 if p is None else order[p]
        if p is not None:
            for h in range(2):
                pairing[2 * p + h][0].wait_recv()
                pairing[2 * p + h][1].wait_recv()

        def slot_tile(i, carry):
            cols = rows_of(i, col)
            rows = arrived[k, :, :, cols].reshape(row_cap, col)
            filled = dot_nn(gather_hot[k], rows).astype(jnp.bfloat16)
            for e in range(exp_dev):
                slots[e, side * capacity : (side + 1) * capacity, cols] = filled[
                    e * capacity : (e + 1) * capacity
                ]
            return carry

        lax.fori_loop(0, width // col, slot_tile, 0, unroll=2)

    wide = 512

    def expert_pass(sources, first_side, low, high):
        sides = slice(first_side * capacity, (first_side + len(sources)) * capacity)

        def one_expert(e, carry):
            rows = slots[e, sides]
            gate_part = dot_nn(rows, wg[e])
            up_part = dot_nn(rows, wu[e])
            weight = jnp.concatenate(
                [
                    slot_weight[0 if p is None else order[p], rows_of(e, capacity), :]
                    for p in sources
                ], axis=0
            )
            hidden = gate_part / (1.0 + jnp.exp(-gate_part)) * up_part * weight
            hidden = hidden.astype(jnp.bfloat16)
            for c in range(width // wide):
                cols = slice(c * wide, (c + 1) * wide)
                result = dot_nn(hidden, wd[e, :, cols]).astype(jnp.bfloat16)
                for i in range(len(sources)):
                    down[first_side + i, e, :, cols] = result[i * capacity : (i + 1) * capacity]
            return carry

        lax.fori_loop(low, high, one_expert, 0, unroll=2)

    back_pairing = {}
    back_crossing = {}
    back_along = {}

    def combine(p, side):
        k = 0 if p is None else order[p]

        def block(c):
            cols = rows_of(c, quarter)
            rows = down[side, :, :, cols].reshape(n_slots, quarter)
            partial[k, c] = dot_nn(return_hot[k], rows).astype(jnp.bfloat16)

        block(pair_across)
        block(pair)
        back_pairing[1, p].start()
        back_pairing[0, p].start()
        block(across)
        block(mine)

    rows_half = row_cap // 2

    def back_cross(p, h):
        k = 0 if p is None else order[p]
        if h == 0:
            back_pairing[1, p].wait_recv()
        rows = slice(h * rows_half, (h + 1) * rows_half)
        partial[k, across, rows] = (
            partial[k, across, rows].astype(jnp.float32) + paired[1, k, rows].astype(jnp.float32)
        ).astype(jnp.bfloat16)
        back_crossing[p, h].start()

    def back_send(p, h):
        k = 0 if p is None else order[p]
        if h == 0:
            back_pairing[0, p].wait_recv()
        back_crossing[p, h].wait_recv()
        rows = slice(h * rows_half, (h + 1) * rows_half)
        total = partial[k, mine, rows].astype(jnp.float32) + paired[0, k, rows].astype(jnp.float32)
        total = (total + crossed[k, rows].astype(jnp.float32)).astype(jnp.bfloat16)
        if p is None:
            returned[0, rows] = total
            return
        partial[k, mine, rows] = total
        back_along[p, h].start()

    for p in (None, 0, 1, 2):
        k = 0 if p is None else order[p]
        for way, side in ((1, pair_across), (0, pair)):
            back_pairing[way, p] = remote(
                partial.at[k, side],
                paired.at[way, k],
                rc_send.at[way, k],
                rc_recv.at[way, k],
                {"tp": pair},
            )
        for h in range(2):
            rows = pl.ds(h * rows_half, rows_half)
            back_crossing[p, h] = remote(
                partial.at[k, across, rows],
                crossed.at[k, rows],
                rx_send.at[k, h],
                rx_recv.at[k, h],
                {"tp": across},
            )
            if p is not None:
                back_along[p, h] = remote(
                    partial.at[k, mine, rows],
                    returned.at[k, rows],
                    rz_send.at[k, h],
                    rz_recv.at[k, h],
                    {"ep": (me + n_ep - k) % n_ep},
                )

    mixer_copies = {
        way: remote(mixp.at[block], mpaired.at[way], m_send.at[way], m_recv.at[way], {"tp": pair})
        for way, block in ((1, pair_across), (0, pair))
    }
    half = span // n_tp // 2
    for h in range(2):
        block = slice(h * half, (h + 1) * half)
        mixer_copies[2 + h] = remote(
            mixp.at[across, block], mcrossed.at[block], m_send.at[2 + h], m_recv.at[2 + h], {"tp": across}
        )

    def mixer_start():
        for h in range(heads):
            att[:, h * head : (h + 1) * head] = (run_acc[h] / run_sum[h]).astype(jnp.bfloat16)

        def project(c, carry):
            cols = rows_of(c, col)
            rows = dot_nn(att[...], wo[:, cols]).astype(jnp.bfloat16)
            mixp[:, :, cols] = rows.reshape(n_tp, span // n_tp, col)
            return carry

        lax.fori_loop(0, width // col, project, 0, unroll=2)
        mixer_copies[1].start()
        mixer_copies[0].start()

    step = 16

    def mixer_cross(h):
        if h == 0:
            mixer_copies[1].wait_recv()

        def add_tile(i, carry):
            rows = pl.ds(pl.multiple_of(h * half + i * step, step), step)
            mixp[across, rows, :] = (
                mixp[across, rows, :].astype(jnp.float32) + mpaired[1, rows, :].astype(jnp.float32)
            ).astype(jnp.bfloat16)
            return carry

        lax.fori_loop(0, half // step, add_tile, 0)
        mixer_copies[2 + h].start()

    outward = []
    for i, (src, dst, size) in enumerate(((mix_ref, mix_hbm, half), (exp_ref, exp_hbm, span // 2))):
        for h in range(2):
            piece = pl.ds(h * size, size)
            outward.append(
                pltpu.make_async_copy(src.at[piece], dst.at[piece], out_sem.at[2 * i + h])
            )

    def mixer_end():
        mixer_copies[0].wait_recv()

        def add_tile(i, carry):
            rows = rows_of(i, step)
            total = mixp[mine, rows, :].astype(jnp.float32) + mpaired[0, rows, :].astype(
                jnp.float32
            )
            mix_ref[rows, :] = (total + mcrossed[rows, :].astype(jnp.float32)).astype(
                jnp.bfloat16
            )
            return carry

        for h in range(2):
            mixer_copies[2 + h].wait_recv()
            lax.fori_loop(h * half // step, (h + 1) * half // step, add_tile, 0, unroll=2)
            outward[h].start()

    outer = jnp.logical_not(inner)
    last = n_ep - 1
    attend(0)
    get_wo.wait()
    only(me == 0, (mixer_start,))
    slot_tables(0, own)
    fill_slots(None, 0)
    split = exp_dev // 2
    for copy in weights[: 3 * split]:
        copy.wait()
    expert_pass((None,), 0, 0, split)
    pass_on(0, 0)
    pass_on(0, 1)
    for copy in weights[3 * split :]:
        copy.wait()
    expert_pass((None,), 0, split, exp_dev)
    combine(None, 0)
    notes_sent[0].wait_recv()
    slot_tables(1, ranks(1))
    only(inner, (pass_on, 1, 0), (pass_on, 1, 1))
    only(outer, (back_cross, None, 0), (back_cross, None, 1))
    for k in range(2, n_ep):
        notes_sent[k - 1].wait_recv()
        slot_tables(k, ranks(k))
    relay(0, 0)
    relay(0, 1)

    @pl.when(inner)
    def _():
        kv_copies[0][1].start()
        fill_slots(0, 0)
        pass_on(2, 0)
        pass_on(2, 1)
        only(me == 1, (kv_forward, 1), (attend, 1))
        relay(1, 0)
        relay(1, 1)
        only(me == 1, (mixer_start,))
        fill_slots(1, 1)
        expert_pass((0, 1), 0, 0, split)
        relay(2, 0)
        relay(2, 1)
        only(me == 2, (back_cross, None, 0), (back_cross, None, 1))
        only(me == 1, (mixer_cross, 0))
        expert_pass((0, 1), 0, split, exp_dev)
        only(me == 2, (kv_forward, 1))
        combine(0, 0)
        combine(1, 1)
        only(me == 1, (back_cross, 0, 0), (back_cross, 0, 1))
        only(me == 2, (back_cross, 1, 0), (back_cross, 1, 1))
        fill_slots(2, 0)
        expert_pass((2,), 0, 0, split)
        only(me == 1, (back_cross, 1, 0), (back_cross, 1, 1), (back_send, 0, 0), (back_send, 0, 1))
        only(me == 1, (back_cross, None, 0), (back_cross, None, 1))
        only(me == 2, (kv_forward, 2))
        only(me == 2, (back_cross, 0, 0), (back_cross, 0, 1), (back_send, 1, 0), (back_send, 1, 1))
        expert_pass((2,), 0, split, exp_dev)
        combine(2, 0)
        only(me == 1, (back_send, 1, 0), (back_send, 1, 1))
        only(me == 2, (back_send, 0, 0), (back_send, 0, 1))
        back_cross(2, 0)
        back_cross(2, 1)
        only(me == 2, (attend, 1), (attend, 2), (mixer_start,))
        back_send(None, 0)
        back_send(None, 1)
        only(me == 1, (mixer_cross, 1))
        back_send(2, 0)
        only(me == 2, (mixer_cross, 0))
        back_send(2, 1)
        only(me == 2, (mixer_cross, 1))

    @pl.when(outer)
    def _():
        fill_slots(0, 1)
        step_of = exp_dev // 4
        only(me == 0, (pass_on, 1, 0))
        expert_pass((0,), 1, 0, 2 * step_of)
        only(me == 0, (pass_on, 1, 1))
        only(me == 3, (pass_on, 1, 0))
        expert_pass((0,), 1, 2 * step_of, 3 * step_of)
        only(me == 0, (pass_on, 2, 0))
        only(me == 3, (pass_on, 1, 1))
        expert_pass((0,), 1, 3 * step_of, exp_dev)
        only(me == 3, (pass_on, 2, 0))
        combine(0, 1)
        pass_on(2, 1)
        only(me == 3, (kv_forward, 1), (attend, 1))
        relay(1, 0)
        relay(1, 1)
        fill_slots(1, 0)
        relay(2, 0)
        relay(2, 1)
        back_cross(0, 0)
        back_cross(0, 1)
        only(me == 0, (mixer_cross, 0))
        fill_slots(2, 1)
        expert_pass((1, 2), 0, 0, exp_dev)
        combine(1, 0)
        back_send(0, 0)
        back_send(0, 1)
        combine(2, 1)
        back_cross(1, 0)
        back_cross(1, 1)
        only(me == 3, (kv_forward, 2), (attend, 2), (kv_forward, 3), (attend, 3))
        back_send(1, 0)
        back_cross(2, 0)
        back_send(1, 1)
        back_cross(2, 1)
        back_send(None, 0)
        back_send(None, 1)
        only(me == 0, (mixer_cross, 1))
        only(me == 3, (mixer_start,))
        back_send(2, 0)
        only(me == 3, (mixer_cross, 0))
        back_send(2, 1)
        only(me == 3, (mixer_cross, 1))

    token_column = jnp.transpose(jnp.broadcast_to(token_key, (8, span)), (1, 0))[:, 0:1]
    for k in range(n_ep):
        base = ((me + k) % n_ep * row_cap).astype(jnp.float32)
        final_hot[k] = one_hot(
            iota_f32((span, row_cap), 1) + base == token_column
        )
    for copy in notes_sent:
        copy.wait_send()
    for d in range(n_ep - 1):

        @pl.when((me >= d) & (me < n_ep - 1))
        def _():
            for copy in kv_copies[d]:
                copy.wait_send()

    for copy in along + crossing + sum(pairing, []):
        copy.wait_send()
    for copy in back_pairing.values():
        copy.wait_send()

    for p in (None, 0, 1, 2):
        k = 0 if p is None else order[p]
        if p == 2:
            only(me < 2, (mixer_end,))
        if p is not None:
            for h in range(2):
                back_along[p, h].wait_recv()

        def output_tile(i, carry):
            rows = rows_of(i, 128)
            total = dot_nn(final_hot[k, rows, :], returned[k])
            if p is not None:
                total = total + exp_acc[rows, :]
            if p == 2:
                exp_ref[rows, :] = total.astype(jnp.bfloat16)
            else:
                exp_acc[rows, :] = total
            return carry

        if p == 2:
            for h in range(2):
                lax.fori_loop(h * span // 256, (h + 1) * span // 256, output_tile, 0, unroll=2)
                outward[2 + h].start()
        else:
            lax.fori_loop(0, span // 128, output_tile, 0, unroll=2)
    only(me > 1, (mixer_end,))

    for copy in outward:
        copy.wait()
    for group in (back_crossing, back_along, mixer_copies):
        for copy in group.values():
            copy.wait_send()


def fused_half(
    queries,
    key_rows,
    value_rows,
    query_gain,
    key_gain,
    log_forget,
    out_weight,
    expert_rows,
    expert_gain,
    routes,
    route_weight,
    gate_weight,
    up_weight,
    down_weight,
    capacity,
):
    n_tp = lax.axis_size("tp")
    n_ep = lax.axis_size("ep")
    span, width = expert_rows.shape
    exp_dev = gate_weight.shape[0]
    hidden = gate_weight.shape[2]
    heads = queries.shape[1] // HEAD_SIZE
    row_cap = exp_dev * capacity // TOP
    part = row_cap // n_tp
    quarter = width // n_tp
    n_slots = exp_dev * capacity
    whole = log_forget.shape[1]
    low = jnp.bfloat16
    full = jnp.float32
    vmem = pltpu.VMEM
    dma = pltpu.SemaphoreType.DMA
    scratch = [
        vmem((span // n_tp, width), low),
        vmem((span, quarter), low),
        vmem((span, heads * HEAD_SIZE), low),
        vmem((span, HEAD_SIZE), low),
        vmem((n_ep, 2, span, HEAD_SIZE), low),
        vmem((1, HEAD_SIZE), full),
        vmem((1, HEAD_SIZE), full),
        vmem((heads, whole), full),
        vmem((heads * HEAD_SIZE, width), low),
        vmem((n_tp, span // n_tp, width), low),
        vmem((1, width), full),
        vmem((TOP, span), jnp.int32),
        vmem((TOP, span), full),
        vmem((n_ep, 8, span), full),
        vmem((exp_dev, width, hidden), low),
        vmem((exp_dev, width, hidden), low),
        vmem((exp_dev, hidden, width), low),
        vmem((heads, span, HEAD_SIZE), low),
        vmem((heads, span, 1), full),
        vmem((heads, span, 1), full),
        vmem((heads, span, HEAD_SIZE), full),
        vmem((span, heads * HEAD_SIZE), low),
        vmem((2, span // n_tp, width), low),
        vmem((span // n_tp, width), low),
        vmem((span, width), low),
        vmem((span, span), low),
        vmem((n_ep - 1, part, width), low),
        vmem((n_ep, n_tp, part, width), low),
        vmem((n_ep, n_slots, row_cap), low),
        vmem((n_ep, row_cap, n_slots), low),
        vmem((n_ep, n_slots, 1), full),
        vmem((n_ep, span, row_cap), low),
        vmem((span, quarter), full),
        vmem((exp_dev, 2 * capacity, width), low),
        vmem((2, exp_dev, capacity, width), low),
        vmem((n_ep, n_tp, row_cap, quarter), low),
        vmem((2, n_ep, row_cap, quarter), low),
        vmem((n_ep, row_cap, quarter), low),
        vmem((n_ep, row_cap, quarter), low),
        dma((14,)),
        dma((3, exp_dev)),
        dma((n_ep, 2)),
        dma((n_ep, 2)),
        dma((n_ep,)),
        dma((n_ep,)),
        dma((n_ep, 2)),
        dma((n_ep, 2)),
        dma((n_ep, 2)),
        dma((n_ep, 2)),
        dma((2, n_ep, 2)),
        dma((2, n_ep, 2)),
        dma((2, n_ep)),
        dma((2, n_ep)),
        dma((n_ep, 2)),
        dma((n_ep, 2)),
        dma((n_ep, 2)),
        dma((n_ep, 2)),
        dma((4,)),
        dma((4,)),
        dma((4,)),
    ]
    mixed, combined = pl.pallas_call(
        functools.partial(fused_kernel, n_ep, n_tp, capacity),
        out_shape=(
            jax.ShapeDtypeStruct((span // n_tp, width), low),
            jax.ShapeDtypeStruct((span, quarter), low),
        ),
        in_specs=[pl.BlockSpec(memory_space=pl.ANY)] * 14,
        out_specs=(
            pl.BlockSpec(memory_space=pltpu.HBM),
            pl.BlockSpec(memory_space=pltpu.HBM),
        ),
        scratch_shapes=scratch,
        compiler_params=pltpu.CompilerParams(
            collective_id=0, has_side_effects=True, vmem_limit_bytes=VMEM_LIMIT
        ),
    )(
        queries,
        key_rows,
        value_rows,
        query_gain.reshape(1, -1),
        key_gain.reshape(1, -1),
        log_forget,
        out_weight,
        expert_rows,
        expert_gain.reshape(1, -1),
        routes,
        route_weight,
        gate_weight,
        up_weight,
        down_weight,
    )
    return settle(mixed, combined)


def settle_kernel(first_in, second_in, first_out, second_out, first, second, sems):
    loads = []
    for i, (src, dst) in enumerate(((first_in, first), (second_in, second))):
        rows = dst.shape[0] // PIECES
        for c in range(PIECES):
            piece = pl.ds(c * rows, rows)
            copy = pltpu.make_async_copy(src.at[piece], dst.at[piece], sems.at[0, i, c])
            copy.start()
            loads.append((i, c, piece, copy))
    stores = []
    for i, c, piece, load in loads:
        load.wait()
        src, dst = ((first, first_out), (second, second_out))[i]
        copy = pltpu.make_async_copy(src.at[piece], dst.at[piece], sems.at[1, i, c])
        copy.start()
        stores.append(copy)
    for copy in stores:
        copy.wait()


def settle(first, second):
    anywhere = pl.BlockSpec(memory_space=pltpu.HBM)
    return pl.pallas_call(
        settle_kernel,
        out_shape=tuple(jax.ShapeDtypeStruct(a.shape, a.dtype) for a in (first, second)),
        in_specs=[anywhere, anywhere],
        out_specs=(anywhere, anywhere),
        scratch_shapes=[
            pltpu.VMEM(first.shape, first.dtype),
            pltpu.VMEM(second.shape, second.dtype),
            pltpu.SemaphoreType.DMA((2, 2, PIECES)),
        ],
        compiler_params=pltpu.CompilerParams(vmem_limit_bytes=VMEM_LIMIT),
    )(first, second)


def on_device(
    queries,
    key_rows,
    value_rows,
    query_gain,
    key_gain,
    log_forget,
    out_weight,
    expert_rows,
    expert_gain,
    routes,
    route_weight,
    gate_weight,
    up_weight,
    down_weight,
):
    mixer_args = (
        queries,
        key_rows,
        value_rows,
        query_gain,
        key_gain,
        log_forget,
        out_weight,
    )
    expert_args = (
        expert_rows,
        expert_gain,
        routes,
        route_weight,
        gate_weight,
        up_weight,
        down_weight,
    )
    n_tp = lax.axis_size("tp")
    n_ep = lax.axis_size("ep")
    span = expert_rows.shape[0]
    capacity = n_tp * ((3 * (span // n_tp) * TOP + 2 * EXPERTS - 1) // (2 * EXPERTS))
    fits = (
        n_tp == 4
        and n_ep == 4
        and gate_weight.shape[0] == GROUP_SIZE
        and capacity % 16 == 0
        and key_rows.shape[1] == HEAD_SIZE
    )
    if fits:
        return fused_half(*mixer_args, *expert_args, capacity)
    expert_out = experts_half(*expert_args)
    mixer_part = mixer_half(*mixer_args)
    mixer_out = lax.psum_scatter(mixer_part, "tp", scatter_dimension=0, tiled=True)
    return (mixer_out, expert_out)


def solution(mesh):
    in_specs = (
        P(("grp", "ep"), "tp"),
        P(("grp", "ep"), "tp"),
        P(("grp", "ep"), "tp"),
        P(),
        P(),
        P("tp", "grp"),
        P("tp", None),
        P(("grp", "ep"), None),
        P(),
        P(None, ("grp", "ep")),
        P(None, ("grp", "ep")),
        P("ep", None, "tp"),
        P("ep", None, "tp"),
        P("ep", "tp", None),
    )
    out_specs = (P(("grp", "ep", "tp"), None), P(("grp", "ep"), "tp"))
    return jax.shard_map(
        on_device, mesh=mesh, in_specs=in_specs, out_specs=out_specs, check_vma=False
    )
```
